512 devices in a mesh: sp: 128 (over z, x, core), tp: 4 (over y).
Axes of the slice: x: 4, y: 4, z: 16, core: 2. Of those that a mesh axis runs over, the one named last changes fastest.
Arguments:
- tokens: bfloat16 [16384, 2048], P(('sp', 'tp')), may hold values from -6 to 6
- input_norm_gain: float32 [2048], replicated, may hold values from 0.1 to 1.9
- convolution_value_weight: bfloat16 [2048, 1024], P('sp', 'tp'), may hold values from -0.125 to 0.125
- convolution_gate_weight: bfloat16 [2048, 1024], P('sp', 'tp'), may hold values from -0.125 to 0.125
- depthwise_filter_taps: float32 [31, 1024], P(None, 'tp'), may hold values from -4 to 4
- channel_norm_gain: float32 [1024], P('tp'), may hold values from 0.1 to 1.9
- channel_norm_bias: float32 [1024], P('tp'), may hold values from -3 to 3
- query_projection_weight: bfloat16 [2048, 1024], P('sp', 'tp'), may hold values from -0.125 to 0.125
- forget_gate_weight: bfloat16 [2048, 1024], P('sp', 'tp'), may hold values from -0.125 to 0.125
- recurrence_value_weight: bfloat16 [2048, 1024], P('sp', 'tp'), may hold values from -0.125 to 0.125
- output_gate_weight: bfloat16 [2048, 1024], P('sp', 'tp'), may hold values from -0.125 to 0.125
- forget_floor_margin: float32 [1024], P('tp'), may hold values from 6.1035156e-06 to 0.1
- decay_jump_terms: float32 [8, 16384], P('tp', 'sp'), may hold values from -0.7 to 0
- head_norm_gain: float32 [1024], P('tp'), may hold values from 0.1 to 1.9
- convolution_output_weight: bfloat16 [1024, 2048], P('tp', 'sp'), may hold values from -0.125 to 0.125
- recurrence_output_weight: bfloat16 [1024, 2048], P('tp', 'sp'), may hold values from -0.125 to 0.125
Outputs:
- mixed: bfloat16 [16384, 2048], P(('sp', 'tp'))
The draws below stay inside these ranges and needn't reach their ends.
All inputs are finite; a program needn't handle non-finite values.
Results may differ from the reference program's by a relative error of at most 0.015.
Values may be sent and summed in bfloat16 or wider, within the bound.
No kernel may reach another device: no remote copies, remote signals or barrier semaphores. Data moves between devices by JAX's collectives and lax.ppermute only.
A program may use at most 64 MiB of HBM per device.

```python
import math
import jax
import jax.numpy as jnp
from jax import lax

D = 2048
CONV_CH = 1024
CONV_W = 31
HG_HEADS = 8
HG_DK = 128
HG_DV = 128
HG_BLOCK = 64
TOK_DEV = 128
TOKENS = 16384
N_TP = 4


def draw_depthwise_filter_taps(key, part):
    noise_key, scale_key = jax.random.split(key, 2)
    channel = jnp.arange(CONV_CH, dtype=jnp.float32) / CONV_CH
    jitter = jax.random.uniform(scale_key, (CONV_CH,), jnp.float32, -1.15, 1.15)
    scales = jnp.exp(math.log(3.0) * channel + jitter) / 3.0
    noise_draw = jax.random.normal(noise_key, (CONV_W, CONV_CH), jnp.float32)
    return jnp.clip(noise_draw * scales / math.sqrt(CONV_W), -4.0, 4.0)


def draw_forget_floor_margin(key, part):
    order_key, slow_key, fast_key = jax.random.split(key, 3)
    order = jax.random.permutation(order_key, HG_HEADS)
    slow_head = jnp.repeat(order < HG_HEADS // 2, HG_DK)
    slow_gap = jnp.exp(jax.random.uniform(slow_key, (HG_HEADS * HG_DK,), jnp.float32, math.log(0.1), math.log(0.5))) / TOKENS
    fast_gap = jnp.exp(jax.random.uniform(fast_key, (HG_HEADS * HG_DK,), jnp.float32, math.log(0.03), math.log(0.1)))
    return jnp.where(slow_head, slow_gap, fast_gap)


def draw_decay_jump_terms(key, part):
    rate_key, place_key, depth_key = jax.random.split(key, 3)
    block_total = TOKENS // TOK_DEV
    third = TOKENS // 3
    rates = jnp.exp(jax.random.uniform(rate_key, (HG_HEADS, block_total), jnp.float32, math.log(0.15), math.log(0.6))) / TOKENS
    decay_depths = jnp.log(jax.random.uniform(depth_key, (HG_HEADS, 2), jnp.float32, 0.55, 0.8))
    place_indices = jax.random.randint(place_key, (HG_HEADS, 2), 0, third) + jnp.arange(2)[None, :] * third
    steady_decay = -jnp.repeat(rates, TOK_DEV, axis=1)
    position_indices = jnp.arange(TOKENS)
    decay_jumps = jnp.sum(jnp.where(position_indices[None, None, :] == place_indices[:, :, None], decay_depths[:, :, None], 0.0), axis=1)
    return steady_decay + decay_jumps


def shard_levels(stream_key, extent, cuts, low, high):
    level, own = 1.0, jax.random.fold_in(stream_key, 6)
    for axis_at, shards_of in cuts:
        draws = jnp.exp(jax.random.uniform(jax.random.fold_in(own, axis_at), (shards_of,), jnp.float32, low / len(cuts), high / len(cuts)))
        level = level * jnp.repeat(draws, extent[axis_at] // shards_of).reshape([-1 if axis == axis_at else 1 for axis in range(len(extent))])
    return level


def scatter_about(rng, extent, scale, bound, cuts=(), held_as=jnp.bfloat16):
    loudness = shard_levels(rng, extent, cuts, -0.22, 0.18) if cuts else 1.0
    entries = jax.random.normal(rng, extent, jnp.float32) * scale * loudness
    return jnp.minimum(jnp.maximum(entries, -bound), bound).astype(held_as)


def setup_inputs(seed: int = 0) -> dict:
    splits = jax.random.split(jax.random.key(seed), 17)
    tokens = scatter_about(splits[0], (TOKENS, D), 1.0, 6.0, ((0, 512),))
    input_norm_gain = jnp.clip(1.0 + 0.18 * jax.random.normal(splits[1], (D,), jnp.float32), 0.1, 1.9)
    convolution_value_weight = scatter_about(splits[2], (D, CONV_CH), D ** -0.5, 0.125, ((0, 128), (1, 4)))
    convolution_gate_weight = scatter_about(splits[3], (D, CONV_CH), D ** -0.5, 0.125, ((0, 128), (1, 4)))
    depthwise_filter_taps = draw_depthwise_filter_taps(jax.random.fold_in(splits[16], 71), 0)
    channel_norm_gain = jnp.clip(1.0 + 0.18 * jax.random.normal(splits[5], (CONV_CH,), jnp.float32), 0.1, 1.9)
    channel_norm_bias = scatter_about(splits[6], (CONV_CH,), 0.5, 3.0, ((0, 4),), jnp.float32)
    query_projection_weight = scatter_about(splits[7], (D, HG_HEADS * HG_DK), D ** -0.5, 0.125, ((0, 128), (1, 4)))
    forget_gate_weight = scatter_about(splits[8], (D, HG_HEADS * HG_DK), D ** -0.5, 0.125, ((0, 128), (1, 4)))
    recurrence_value_weight = scatter_about(splits[9], (D, HG_HEADS * HG_DV), D ** -0.5, 0.125, ((0, 128), (1, 4)))
    output_gate_weight = scatter_about(splits[10], (D, HG_HEADS * HG_DV), D ** -0.5, 0.125, ((0, 128), (1, 4)))
    forget_floor_margin = draw_forget_floor_margin(jax.random.fold_in(splits[16], 71), 0)
    decay_jump_terms = draw_decay_jump_terms(jax.random.fold_in(splits[16], 71), 0)
    head_norm_gain = jnp.clip(1.0 + 0.18 * jax.random.normal(splits[13], (HG_HEADS * HG_DV,), jnp.float32), 0.1, 1.9)
    convolution_output_weight = scatter_about(splits[14], (CONV_CH, D), (CONV_CH + HG_HEADS * HG_DV) ** -0.5, 0.125, ((0, 4), (1, 128)))
    recurrence_output_weight = scatter_about(splits[15], (HG_HEADS * HG_DV, D), (CONV_CH + HG_HEADS * HG_DV) ** -0.5, 0.125, ((0, 4), (1, 128)))
    return {"tokens": tokens, "input_norm_gain": input_norm_gain, "convolution_value_weight": convolution_value_weight, "convolution_gate_weight": convolution_gate_weight, "depthwise_filter_taps": depthwise_filter_taps, "channel_norm_gain": channel_norm_gain, "channel_norm_bias": channel_norm_bias, "query_projection_weight": query_projection_weight, "forget_gate_weight": forget_gate_weight, "recurrence_value_weight": recurrence_value_weight, "output_gate_weight": output_gate_weight, "forget_floor_margin": forget_floor_margin, "decay_jump_terms": decay_jump_terms, "head_norm_gain": head_norm_gain, "convolution_output_weight": convolution_output_weight, "recurrence_output_weight": recurrence_output_weight}


norm_eps = 1e-06
layer_eps = 1e-05
highest_precision = lax.Precision.HIGHEST

def convolve(gated, kernel):
    return lax.conv_general_dilated(gated[None], kernel[:, None, :], (1,), 'VALID', dimension_numbers=('NWC', 'WIO', 'NWC'), feature_group_count=gated.shape[1], precision=highest_precision)[0]

def channel_norm(values, first_sum, second_sum, gain, bias):
    mean_value = first_sum[:, None] / CONV_CH
    variance = second_sum[:, None] / CONV_CH - mean_value * mean_value
    shifted = (values - mean_value) * lax.rsqrt(variance + layer_eps) * gain + bias
    return jax.nn.silu(shifted).astype(jnp.bfloat16)

def gate_factors(query_projected, forget_projected, forget_floor_margin, decay_jump_rows):
    row_total_count = query_projected.shape[0]
    head_total_count = decay_jump_rows.shape[1]
    query_rows = jax.nn.silu(query_projected.astype(jnp.float32))
    log_forget_gate = jnp.logaddexp(jnp.log1p(-forget_floor_margin), jnp.log(forget_floor_margin) + jax.nn.log_sigmoid(forget_projected.astype(jnp.float32)))
    key_gate_values = -jnp.expm1(log_forget_gate)
    log_decay_running = log_forget_gate.reshape(row_total_count, head_total_count, -1) + decay_jump_rows[:, :, None]
    return (query_rows.reshape(row_total_count, head_total_count, -1), key_gate_values.reshape(row_total_count, head_total_count, -1), log_decay_running)

def finish(recurrent, gain, outgate_proj):
    row_total_count = recurrent.shape[0]
    scaled = recurrent * lax.rsqrt(lax.optimization_barrier(jnp.mean(recurrent * recurrent, axis=2, keepdims=True)) + norm_eps)
    gated_out = scaled.reshape(row_total_count, -1) * gain * jax.nn.silu(outgate_proj.astype(jnp.float32))
    return gated_out.astype(jnp.bfloat16)

def block_step(recurrence_state, block_parts):
    query_rows, key_gate_values, input_rows, log_decay_running = block_parts
    block_len = query_rows.shape[1]
    cumulative = jnp.cumsum(log_decay_running, axis=1)
    final_decay = cumulative[:, -1:, :]
    query_rows_scaled = query_rows * jnp.exp(cumulative)
    scaled_keys = key_gate_values * jnp.exp(-cumulative)
    final_keys = key_gate_values * jnp.exp(final_decay - cumulative)
    attention_scores = jnp.einsum('htk,hsk->hts', query_rows_scaled, scaled_keys, precision=highest_precision)
    causal = jnp.arange(block_len)[:, None] >= jnp.arange(block_len)[None, :]
    attention_scores = jnp.where(causal[None], attention_scores, 0.0)
    output_rows = jnp.einsum('mby,myx->mbx', attention_scores, input_rows, precision=highest_precision) + jnp.einsum('ufi,uij->ufj', query_rows_scaled, recurrence_state, precision=highest_precision)
    recurrence_state = jnp.exp(final_decay[:, 0, :])[:, :, None] * recurrence_state + jnp.einsum('meg,met->mgt', final_keys, input_rows, precision=highest_precision)
    return (recurrence_state, output_rows)

def reference(tokens, input_norm_gain, convolution_value_weight, convolution_gate_weight, depthwise_filter_taps, channel_norm_gain, channel_norm_bias, query_projection_weight, forget_gate_weight, recurrence_value_weight, output_gate_weight, forget_floor_margin, decay_jump_terms, head_norm_gain, convolution_output_weight, recurrence_output_weight):
    features = tokens.astype(jnp.float32)
    normed = (features * lax.rsqrt(lax.optimization_barrier(jnp.mean(features * features, axis=1, keepdims=True)) + norm_eps) * input_norm_gain).astype(jnp.bfloat16)

    def project(weight):
        return jnp.dot(normed, weight, preferred_element_type=jnp.float32).astype(jnp.bfloat16)
    value_proj = project(convolution_value_weight)
    gate_proj = project(convolution_gate_weight)
    query_projected = project(query_projection_weight)
    forget_projected = project(forget_gate_weight)
    input_proj = project(recurrence_value_weight)
    outgate_proj = project(output_gate_weight)
    gated = value_proj.astype(jnp.float32) * jax.nn.sigmoid(gate_proj.astype(jnp.float32))
    padded = jnp.pad(gated, ((CONV_W - 1, 0), (0, 0)))
    convolved = convolve(padded, depthwise_filter_taps).astype(jnp.bfloat16)
    values = convolved.astype(jnp.float32)
    conv_out = channel_norm(values, lax.optimization_barrier(jnp.sum(values, axis=1)), lax.optimization_barrier(jnp.sum(values * values, axis=1)), channel_norm_gain, channel_norm_bias)
    query_rows, key_gate_values, log_decay_running = gate_factors(query_projected, forget_projected, forget_floor_margin, decay_jump_terms.T)
    input_rows = input_proj.astype(jnp.float32).reshape(TOKENS, HG_HEADS, HG_DV)
    block_count = TOKENS // HG_BLOCK

    def to_blocks(array):
        return array.reshape(block_count, HG_BLOCK, HG_HEADS, -1).transpose(0, 2, 1, 3)
    initial = jnp.zeros((HG_HEADS, HG_DK, HG_DV), jnp.float32)
    scanned = lax.scan(block_step, initial, (to_blocks(query_rows), to_blocks(key_gate_values), to_blocks(input_rows), to_blocks(log_decay_running)))
    recurrent = scanned[1].transpose(0, 2, 1, 3).reshape(TOKENS, HG_HEADS, HG_DV)
    rec_out = finish(recurrent, head_norm_gain, outgate_proj)
    conv_group = CONV_CH // N_TP
    rec_group = HG_HEADS * HG_DV // N_TP
    summed = jnp.zeros((TOKENS, D), jnp.float32)
    for group in range(N_TP):
        conv_slice = slice(group * conv_group, (group + 1) * conv_group)
        rec_slice = slice(group * rec_group, (group + 1) * rec_group)
        partial_sum = jnp.dot(conv_out[:, conv_slice], convolution_output_weight[conv_slice], preferred_element_type=jnp.float32) + jnp.dot(rec_out[:, rec_slice], recurrence_output_weight[rec_slice], preferred_element_type=jnp.float32)
        summed = summed + lax.optimization_barrier(partial_sum.astype(jnp.bfloat16)).astype(jnp.float32)
    return summed.astype(jnp.bfloat16)
```

```python
import jax
import jax.numpy as jnp
from jax import lax
from jax.experimental import pallas as pl
from jax.experimental.pallas import tpu as pltpu
from jax.sharding import Mesh
from jax.sharding import PartitionSpec as P

Z, X, C, Y = "sp_0", "sp_1", "sp_2", "tp"
SP = (Z, X, C)
SP_TP = (Z, X, C, Y)
NZ, NX, NC, NY = 16, 4, 2, 4
CONV_CH = 1024
CH = 128
ROWS = 256
OWN = 32
BLOCK = 64
TAPS = 31
HALO = 32
STATE_ROWS = 40
norm_eps = 1e-06
layer_eps = 1e-05
HIGH = lax.Precision.HIGHEST
bf16 = jnp.bfloat16
f32 = jnp.float32

VMEM = pl.BlockSpec(memory_space=pltpu.VMEM)
SMEM = pl.BlockSpec(memory_space=pltpu.SMEM)


def kernel_call(body, out, specs, scratch=(), name=None):
    return pl.pallas_call(
        body,
        out_shape=out,
        in_specs=specs,
        out_specs=jax.tree.map(lambda _: VMEM, out),
        scratch_shapes=scratch,
        name=name,
    )


def shape(dims, dtype):
    return jax.ShapeDtypeStruct(dims, dtype)


def matmul(a, b, dims, precision=None):
    return lax.dot_general(
        a, b, (dims, ((), ())), precision=precision, preferred_element_type=f32
    )


def sigmoid(v):
    return 1.0 / (1.0 + jnp.exp(-v))


def silu(v):
    return v * sigmoid(v)


def lane_groups(shape_of):
    return lax.broadcasted_iota(jnp.int32, shape_of, 1) // 32


def own_half(value, core):
    return jnp.where(core == 0, value[:, :CH], value[:, CH:])


def norm_body(tokens, gain, out):
    features = tokens[...].astype(f32)
    normed = (
        features
        * lax.rsqrt(jnp.mean(features * features, axis=1, keepdims=True) + norm_eps)
        * gain[...]
    )
    group = lane_groups((OWN, CH))
    for x in range(NX):
        for j in range(NZ // 4):
            piece = jnp.zeros((OWN, CH), f32)
            for i in range(4):
                at = (4 * j + i) * CH
                source = normed[:, at : at + CH]
                turned = pltpu.roll(source, (32 * (i - x)) % CH, 1) if i != x else source
                piece = jnp.where(group == i, turned, piece)
            to = (x * 4 + j) * CH
            out[:, to : to + CH] = piece.astype(bf16)


def in_order(value):
    pieces = [
        value[(y * NC + c) * OWN : (y * NC + c + 1) * OWN] for c in range(NC) for y in range(NY)
    ]
    return jnp.concatenate(pieces, axis=0)


def local_body(core, projected, margin, jump, inner, decayed, packed):
    c = core[0]
    bound = own_half(margin[...], c)
    both = in_order(projected[...]).astype(f32)
    queries = silu(both[:, :CH])
    keys = bound * sigmoid(-both[:, CH : 2 * CH])
    log_forget = jnp.log1p(-keys)
    inputs = both[:, 2 * CH :].astype(bf16)
    row = lax.broadcasted_iota(jnp.int32, (BLOCK, BLOCK), 0)
    col = lax.broadcasted_iota(jnp.int32, (BLOCK, BLOCK), 1)
    causal = row >= col
    lower = jnp.where(causal, 1.0, 0.0)
    state = jnp.zeros((CH, CH), f32)
    before = jnp.zeros((1, CH), f32)
    for n in range(ROWS // BLOCK):
        at = slice(n * BLOCK, (n + 1) * BLOCK)
        jumps = jump[:, n * BLOCK : (n + 1) * BLOCK]
        jumped = jnp.sum(jnp.where(causal, jumps, 0.0), axis=1, keepdims=True)
        running = matmul(lower, log_forget[at], ((1,), (0,)), HIGH) + jumped
        final = running[BLOCK - 1 : BLOCK]
        scaled = queries[at] * jnp.exp(running)
        scaled_keys = (keys[at] * jnp.exp(-running)).astype(bf16)
        final_keys = (keys[at] * jnp.exp(final - running)).astype(bf16)
        scores = matmul(scaled.astype(bf16), scaled_keys, ((1,), (1,)))
        scores = jnp.where(causal, scores, 0.0).astype(bf16)
        inner[at] = matmul(scores, inputs[at], ((1,), (0,))) + matmul(
            scaled.astype(bf16), state.astype(bf16), ((1,), (1,))
        )
        decayed[at] = (scaled * jnp.exp(before)).astype(bf16)
        state = state * jnp.exp(final) + matmul(inputs[at], final_keys, ((0,), (0,)))
        before = before + final
    high = before.astype(bf16)
    low = (before - high.astype(f32)).astype(bf16)
    first = lax.broadcasted_iota(jnp.int32, (8, CH), 0)
    tail = jnp.where(first == 0, high.astype(f32), jnp.where(first == 1, low.astype(f32), 0.0))
    for x in range(NX):
        packed[x, :OWN] = state[x * OWN : (x + 1) * OWN].astype(bf16)
        packed[x, OWN:] = tail.astype(bf16)


def unpacked(block):
    wide = block.astype(f32)
    return wide[OWN : OWN + 1] + wide[OWN + 1 : OWN + 2], wide[:OWN]


def slab_body(parts, total):
    state = jnp.zeros((OWN, CH), f32)
    decay = jnp.zeros((1, CH), f32)
    for x in range(NX):
        step, add = unpacked(parts[x])
        state = state * jnp.exp(step) + add
        decay = decay + step
    high = decay.astype(bf16).astype(f32)
    low = decay - high
    first = lax.broadcasted_iota(jnp.int32, (8, CH), 0)
    total[:OWN] = state.astype(bf16)
    total[OWN:] = jnp.where(first == 0, high, jnp.where(first == 1, low, 0.0)).astype(bf16)


def prefix_body(place, slabs, parts, starts):
    mine = place[0]
    state = jnp.zeros((OWN, CH), f32)
    for z in range(NZ):
        step, add = unpacked(slabs[z])
        state = jnp.where(z < mine, state * jnp.exp(step) + add, state)
    for x in range(NX):
        starts[x] = state.astype(bf16)
        step, add = unpacked(parts[x])
        state = state * jnp.exp(step) + add


def finish_body(core, inner, decayed, start, gain, outgate, out):
    recurrent = inner[...] + matmul(decayed[...], start[...], ((1,), (1,)))
    scale = lax.rsqrt(jnp.mean(recurrent * recurrent, axis=1, keepdims=True) + norm_eps)
    gate = silu(in_order(outgate[...]).astype(f32))
    out[...] = (recurrent * scale * own_half(gain[...], core[0]) * gate).astype(bf16)


def conv_body(core, projected, halo, taps, out, sums, gated):
    rim = halo[...].astype(f32)
    gated[:HALO] = rim[:, :CH] * sigmoid(rim[:, CH:])
    both = in_order(projected[...]).astype(f32)
    gated[HALO:] = both[:, :CH] * sigmoid(both[:, CH:])
    own_taps = own_half(taps[...], core[0])
    for n in range(ROWS // BLOCK):
        total = jnp.zeros((BLOCK, CH), f32)
        for j in range(TAPS):
            at = n * BLOCK + HALO - TAPS + 1 + j
            total = total + gated[at : at + BLOCK] * own_taps[j : j + 1]
        out[n * BLOCK : (n + 1) * BLOCK] = total.astype(bf16)
    values = out[...].astype(f32)
    ones = jnp.ones((8, CH), f32)
    first_sum = matmul(ones, values, ((1,), (1,)), HIGH)
    second_sum = matmul(ones, values * values, ((1,), (1,)), HIGH)
    row = lax.broadcasted_iota(jnp.int32, (8, ROWS), 0)
    both_sums = jnp.where(row == 0, first_sum, second_sum)
    for k in range(NC * NY):
        sums[k] = both_sums


def channel_body(core, values, sums, gain, bias, out):
    total = sums[0]
    for k in range(1, NC * NY):
        total = total + sums[k]
    row = lax.broadcasted_iota(jnp.int32, (8, CH), 0)
    pick_first = jnp.where(row == 0, 1.0 / CONV_CH, 0.0)
    pick_second = jnp.where(row == 1, 1.0 / CONV_CH, 0.0)
    mean = matmul(total, pick_first, ((0,), (0,)), HIGH)
    variance = matmul(total, pick_second, ((0,), (0,)), HIGH) - mean * mean
    shifted = (values[...].astype(f32) - mean) * lax.rsqrt(variance + layer_eps)
    out[...] = silu(
        shifted * own_half(gain[...], core[0]) + own_half(bias[...], core[0])
    ).astype(bf16)


def last_body(parts, out):
    total = parts[0].astype(f32)
    for y in range(1, NY):
        total = total + parts[y].astype(f32)
    group = lane_groups((OWN, CH))
    for z in range(NZ):
        piece = jnp.zeros((OWN, CH), f32)
        for x in range(NX):
            at = (x * 4 + z // 4) * CH
            source = total[:, at : at + CH]
            shift = (32 * (x - z % 4)) % CH
            turned = pltpu.roll(source, shift, 1) if shift else source
            piece = jnp.where(group == x, turned, piece)
        out[:, z * CH : (z + 1) * CH] = piece.astype(bf16)


def exchanged(x, axes):
    return lax.all_to_all(x, axes, split_axis=0, concat_axis=0, tiled=True)


def to_everyone(x, axes):
    return exchanged(jnp.broadcast_to(x, (lax.axis_size(axes), *x.shape)), axes)


def per_device(
    tokens,
    input_norm_gain,
    convolution_value_weight,
    convolution_gate_weight,
    depthwise_filter_taps,
    channel_norm_gain,
    channel_norm_bias,
    query_projection_weight,
    forget_gate_weight,
    recurrence_value_weight,
    output_gate_weight,
    forget_floor_margin,
    decay_jump_terms,
    head_norm_gain,
    convolution_output_weight,
    recurrence_output_weight,
):
    core = lax.axis_index(C).astype(jnp.int32).reshape(1)
    place = lax.axis_index(Z).astype(jnp.int32).reshape(1)
    width = tokens.shape[1]

    normed = kernel_call(norm_body, shape((OWN, width), bf16), [VMEM, VMEM], name="norm")(
        tokens, input_norm_gain.reshape(1, width)
    )

    weights = (
        query_projection_weight,
        forget_gate_weight,
        recurrence_value_weight,
        convolution_value_weight,
        convolution_gate_weight,
        output_gate_weight,
        convolution_output_weight.T,
        recurrence_output_weight.T,
    )
    jump_high = decay_jump_terms.astype(bf16)
    jump_low = (decay_jump_terms - jump_high.astype(f32)).astype(bf16)
    payload = []
    for c in range(NC):
        half = jnp.concatenate([w[:, c * CH : (c + 1) * CH] for w in weights], axis=1)
        jumps = jnp.concatenate([jump_high[c], jump_low[c]])
        payload.append(
            jnp.concatenate(
                [
                    normed,
                    jnp.concatenate([half[:8], half[8:]], axis=1),
                    jnp.broadcast_to(jnp.tile(jumps, 8), (8, width)),
                ],
                axis=0,
            )
        )
    arrived = exchanged(jnp.stack(payload), C)

    jumps = arrived[:, 40, : 2 * CH].astype(f32)
    jump = (jumps[:, :CH] + jumps[:, CH:]).reshape(1, ROWS)
    pair = arrived[:, 32:40]
    shard = jnp.concatenate([pair[:, :, :1024], pair[:, :, 1024:]], axis=1).reshape(32, 1024)
    rows = to_everyone(arrived[:, :32].reshape(2 * OWN, width), Y).reshape(ROWS, width)

    along = lax.all_gather(shard[:, :768], Z, axis=0, tiled=True)
    rec_weight = to_everyone(along[:, :384], X).reshape(width, 384)
    conv_weight = to_everyone(along[:, 384:768], X).reshape(width, 384)
    out_weight = to_everyone(
        to_everyone(shard[:, 768:], Z).reshape(512, 256), X
    ).reshape(width, 256)

    rec_projected = jnp.dot(rows, rec_weight, preferred_element_type=f32).astype(bf16)
    margin = forget_floor_margin.reshape(1, 2 * CH)
    inner, decayed, packed = kernel_call(
        local_body,
        (shape((ROWS, CH), f32), shape((ROWS, CH), bf16), shape((NX, STATE_ROWS, CH), bf16)),
        [SMEM, VMEM, VMEM, VMEM],
        name="local",
    )(core, rec_projected, margin, jump)
    parts = exchanged(packed, X)
    total = kernel_call(slab_body, shape((STATE_ROWS, CH), bf16), [VMEM], name="slab")(parts)
    slabs = to_everyone(total, Z)
    starts = kernel_call(
        prefix_body, shape((NX, OWN, CH), bf16), [SMEM, VMEM, VMEM], name="prefix"
    )(place, slabs, parts)
    start = exchanged(starts, X).reshape(CH, CH)

    conv_projected = jnp.dot(rows, conv_weight, preferred_element_type=f32).astype(bf16)
    value_gate = conv_projected[:, : 2 * CH]
    chips = NZ * NX
    halo = lax.ppermute(
        value_gate[ROWS - HALO :], (Z, X), [(k, k + 1) for k in range(chips - 1)]
    )
    convolved, sums = kernel_call(
        conv_body,
        (shape((ROWS, CH), bf16), shape((NC * NY, 8, ROWS), f32)),
        [SMEM, VMEM, VMEM, VMEM],
        [pltpu.VMEM((HALO + ROWS, CH), f32)],
        name="conv",
    )(core, value_gate, halo, depthwise_filter_taps)
    all_sums = exchanged(sums, (C, Y))
    conv_out = kernel_call(
        channel_body, shape((ROWS, CH), bf16), [SMEM, VMEM, VMEM, VMEM, VMEM], name="channel"
    )(
        core,
        convolved,
        all_sums,
        channel_norm_gain.reshape(1, 2 * CH),
        channel_norm_bias.reshape(1, 2 * CH),
    )
    rec_out = kernel_call(
        finish_body, shape((ROWS, CH), bf16), [SMEM, VMEM, VMEM, VMEM, VMEM, VMEM], name="finish"
    )(core, inner, decayed, start, head_norm_gain.reshape(1, 2 * CH), conv_projected[:, 2 * CH :])

    both = jnp.concatenate([conv_out, rec_out], axis=1)
    partial = matmul(both, out_weight, ((1,), (1,))).astype(bf16).reshape(NC, ROWS // NC, width)
    pair_sum = exchanged(partial, C).astype(f32).sum(axis=0).astype(bf16)
    pieces = exchanged(pair_sum.reshape(NY, OWN, width), Y)
    return kernel_call(last_body, shape((OWN, width), bf16), [VMEM], name="last")(pieces)


def solution(mesh):
    split = Mesh(mesh.devices.reshape(NZ, NX, NC, mesh.shape["tp"]), SP_TP)
    return jax.shard_map(
        per_device,
        mesh=split,
        in_specs=(
            P(SP_TP, None),
            P(),
            P(SP, "tp"),
            P(SP, "tp"),
            P(None, "tp"),
            P("tp"),
            P("tp"),
            P(SP, "tp"),
            P(SP, "tp"),
            P(SP, "tp"),
            P(SP, "tp"),
            P("tp"),
            P("tp", SP),
            P("tp"),
            P("tp", SP),
            P("tp", SP),
        ),
        out_specs=P(SP_TP, None),
        check_vma=False,
    )
```

```python
import jax
import jax.numpy as jnp
from jax import lax
from jax.experimental import pallas as pl
from jax.experimental.pallas import tpu as pltpu
from jax.sharding import Mesh
from jax.sharding import PartitionSpec as P


ZH, ZL, X, C, Y = "sp_0", "sp_1", "sp_2", "sp_3", "tp"
SP = (ZH, ZL, X, C)
SP_TP = (ZH, ZL, X, C, Y)
NZ, NQ, NX, NC, NY = 16, 4, 4, 2, 4
CONV_CH = 1024
CH = 128
ROWS = 256
OWN = 32
BLOCK = 64
TAPS = 31
HALO = 32
STATE_ROWS = 136
PAIR = 64
norm_eps = 1e-06
layer_eps = 1e-05
HIGH = lax.Precision.HIGHEST
bf16 = jnp.bfloat16
f32 = jnp.float32

VMEM = pl.BlockSpec(memory_space=pltpu.VMEM)
SMEM = pl.BlockSpec(memory_space=pltpu.SMEM)


def kernel_call(body, out, specs, scratch=()):
    return pl.pallas_call(
        body,
        out_shape=out,
        in_specs=specs,
        out_specs=jax.tree.map(lambda _: VMEM, out),
        scratch_shapes=scratch,
    )


def shape(dims, dtype):
    return jax.ShapeDtypeStruct(dims, dtype)


def matmul(a, b, dims, precision=None):
    return lax.dot_general(
        a, b, (dims, ((), ())), precision=precision, preferred_element_type=f32
    )


def sigmoid(v):
    return 1.0 / (1.0 + jnp.exp(-v))


def silu(v):
    return v * sigmoid(v)


def lane_groups(shape_of):
    return lax.broadcasted_iota(jnp.int32, shape_of, 1) // 32


def own_half(value, core):
    return jnp.where(core == 0, value[:, :CH], value[:, CH:])


def prepare_body(tokens, gain, query, forget, value, left, gate, outgate, conv_out, rec_out, jump, out):
    features = tokens[...].astype(f32)
    normed = (
        features
        * lax.rsqrt(jnp.mean(features * features, axis=1, keepdims=True) + norm_eps)
        * gain[...]
    )
    group = lane_groups((OWN, CH))
    for x in range(NX):
        for j in range(NZ // 4):
            piece = jnp.zeros((OWN, CH), f32)
            for i in range(4):
                at = (4 * j + i) * CH
                source = normed[:, at : at + CH]
                turned = pltpu.roll(source, (32 * (i - x)) % CH, 1) if i != x else source
                piece = jnp.where(group == i, turned, piece)
            to = (x * 4 + j) * CH
            for c in range(NC):
                out[c, :OWN, to : to + CH] = piece.astype(bf16)
    side = 2 * CH
    same = (
        lax.broadcasted_iota(jnp.int32, (side, side), 0)
        == lax.broadcasted_iota(jnp.int32, (side, side), 1)
    )
    identity = jnp.where(same, 1.0, 0.0).astype(bf16)
    blocks = [w[...].astype(f32) for w in (query, forget, value, left, gate, outgate)]
    blocks += [matmul(w[...], identity, ((0,), (0,))) for w in (conv_out, rec_out)]
    for c in range(NC):
        for k, block in enumerate(blocks):
            half = block[:, c * CH : (c + 1) * CH].astype(bf16)
            out[c, OWN : OWN + 8, k * CH : (k + 1) * CH] = half[:8]
            out[c, OWN : OWN + 8, (8 + k) * CH : (9 + k) * CH] = half[8:]
        row = jnp.broadcast_to(jump[c : c + 1], (8, CH))
        high = row.astype(bf16)
        out[c, OWN + 8 :, :CH] = high
        out[c, OWN + 8 :, CH : 2 * CH] = (row - high.astype(f32)).astype(bf16)
        out[c, OWN + 8 :, 2 * CH :] = jnp.zeros((8, 14 * CH), bf16)


def in_order(ref, y):
    pieces = []
    for c in range(NC):
        for k in range(NY):
            slot = lax.rem(k - y + NY, NY)
            at = pl.multiple_of(slot * PAIR + c * OWN, OWN)
            pieces.append(ref[pl.ds(at, OWN)])
    return jnp.concatenate(pieces, axis=0)


def local_body(place, own, next_one, across, last_one, weight, margin, jump, inner, decayed, packed, projected):
    c = place[3]
    for k, piece in enumerate((own, next_one, across, last_one)):
        projected[k * PAIR : (k + 1) * PAIR] = matmul(piece[...], weight[...], ((1,), (0,)))
    bound = own_half(margin[...], c)
    both = in_order(projected, place[4]).astype(bf16).astype(f32)
    queries = silu(both[:, :CH])
    keys = bound * sigmoid(-both[:, CH : 2 * CH])
    log_forget = jnp.log1p(-keys)
    inputs = both[:, 2 * CH :].astype(bf16)
    row = lax.broadcasted_iota(jnp.int32, (BLOCK, BLOCK), 0)
    col = lax.broadcasted_iota(jnp.int32, (BLOCK, BLOCK), 1)
    causal = row >= col
    lower = jnp.where(causal, 1.0, 0.0)
    state = jnp.zeros((CH, CH), f32)
    before = jnp.zeros((1, CH), f32)
    for n in range(ROWS // BLOCK):
        at = slice(n * BLOCK, (n + 1) * BLOCK)
        jumps = jump[:, n * BLOCK : (n + 1) * BLOCK]
        jumped = jnp.sum(jnp.where(causal, jumps, 0.0), axis=1, keepdims=True)
        running = matmul(lower, log_forget[at], ((1,), (0,)), HIGH) + jumped
        final = running[BLOCK - 1 : BLOCK]
        scaled = queries[at] * jnp.exp(running)
        scaled_keys = (keys[at] * jnp.exp(-running)).astype(bf16)
        final_keys = (keys[at] * jnp.exp(final - running)).astype(bf16)
        scores = matmul(scaled.astype(bf16), scaled_keys, ((1,), (1,)))
        scores = jnp.where(causal, scores, 0.0).astype(bf16)
        inner[at] = matmul(scores, inputs[at], ((1,), (0,))) + matmul(
            scaled.astype(bf16), state.astype(bf16), ((1,), (1,))
        )
        decayed[at] = (scaled * jnp.exp(before)).astype(bf16)
        state = state * jnp.exp(final) + matmul(inputs[at], final_keys, ((0,), (0,)))
        before = before + final
    pack(packed, state, before)


def pack(ref, state, decay):
    high = decay.astype(bf16).astype(f32)
    low = decay - high
    first = lax.broadcasted_iota(jnp.int32, (8, CH), 0)
    ref[:CH] = state.astype(bf16)
    ref[CH:] = jnp.where(first == 0, high, jnp.where(first == 1, low, 0.0)).astype(bf16)


def unpacked(block):
    wide = block.astype(f32)
    return wide[CH : CH + 1] + wide[CH + 1 : CH + 2], wide[:CH]


def total_body(parts, total):
    state = jnp.zeros((CH, CH), f32)
    decay = jnp.zeros((1, CH), f32)
    for k in range(NQ):
        step, add = unpacked(parts[k])
        state = state * jnp.exp(step) + add
        decay = decay + step
    pack(total, state, decay)


def finish_body(place, quads, slabs, chips, inner, decayed, gain, outgate, out):
    state = jnp.zeros((CH, CH), f32)
    for level, parts in enumerate((quads, slabs, chips)):
        for k in range(NQ):
            step, add = unpacked(parts[k])
            state = jnp.where(k < place[level], state * jnp.exp(step) + add, state)
    recurrent = inner[...] + matmul(decayed[...], state.astype(bf16), ((1,), (1,)))
    scale = lax.rsqrt(jnp.mean(recurrent * recurrent, axis=1, keepdims=True) + norm_eps)
    gate = silu(outgate[...].astype(f32))
    out[...] = (recurrent * scale * own_half(gain[...], place[3]) * gate).astype(bf16)


def project_body(place, own, next_one, across, last_one, weight, value_gate, outgate, tail, projected):
    for k, piece in enumerate((own, next_one, across, last_one)):
        projected[k * PAIR : (k + 1) * PAIR] = matmul(piece[...], weight[...], ((1,), (0,)))
    ordered = in_order(projected, place[4]).astype(bf16)
    value_gate[...] = ordered[:, : 2 * CH]
    outgate[...] = ordered[:, 2 * CH :]
    tail[...] = ordered[ROWS - HALO :, : 2 * CH]


def conv_body(place, projected, halo, taps, out, sums, gated):
    rim = halo[...].astype(f32)
    gated[:HALO] = rim[:, :CH] * sigmoid(rim[:, CH:])
    both = projected[...].astype(f32)
    gated[HALO:] = both[:, :CH] * sigmoid(both[:, CH:])
    own_taps = own_half(taps[...], place[3])
    for n in range(ROWS // BLOCK):
        total = jnp.zeros((BLOCK, CH), f32)
        for j in range(TAPS):
            at = n * BLOCK + HALO - TAPS + 1 + j
            total = total + gated[at : at + BLOCK] * own_taps[j : j + 1]
        out[n * BLOCK : (n + 1) * BLOCK] = total.astype(bf16)
    values = out[...].astype(f32)
    ones = jnp.ones((8, CH), f32)
    first_sum = matmul(ones, values, ((1,), (1,)), HIGH)
    second_sum = matmul(ones, values * values, ((1,), (1,)), HIGH)
    row = lax.broadcasted_iota(jnp.int32, (8, ROWS), 0)
    sums[...] = jnp.where(row == 0, first_sum, second_sum)


def channel_body(place, values, sums, gain, bias, out):
    total = sums[0]
    for k in range(1, NC * NY):
        total = total + sums[k]
    row = lax.broadcasted_iota(jnp.int32, (8, CH), 0)
    pick_first = jnp.where(row == 0, 1.0 / CONV_CH, 0.0)
    pick_second = jnp.where(row == 1, 1.0 / CONV_CH, 0.0)
    mean = matmul(total, pick_first, ((0,), (0,)), HIGH)
    variance = matmul(total, pick_second, ((0,), (0,)), HIGH) - mean * mean
    shifted = (values[...].astype(f32) - mean) * lax.rsqrt(variance + layer_eps)
    out[...] = silu(
        shifted * own_half(gain[...], place[3]) + own_half(bias[...], place[3])
    ).astype(bf16)


def output_body(place, conv_out, rec_out, own, next_one, across, last_one, out):
    both = jnp.concatenate([conv_out[...], rec_out[...]], axis=1)
    step = own.shape[0]
    for k, piece in enumerate((own, next_one, across, last_one)):
        result = matmul(both, piece[...], ((1,), (1,))).astype(bf16)
        at = pl.multiple_of(lax.rem(place[2] + k, NX) * step, step)
        for c in range(NC):
            out[c, :, pl.ds(at, step)] = result[c * (ROWS // NC) : (c + 1) * (ROWS // NC)]


def last_body(parts, out):
    total = parts[0].astype(f32)
    for y in range(1, NY):
        total = total + parts[y].astype(f32)
    group = lane_groups((OWN, CH))
    for z in range(NZ):
        piece = jnp.zeros((OWN, CH), f32)
        for x in range(NX):
            at = (x * 4 + z // 4) * CH
            source = total[:, at : at + CH]
            shift = (32 * (x - z % 4)) % CH
            turned = pltpu.roll(source, shift, 1) if shift else source
            piece = jnp.where(group == x, turned, piece)
        out[:, z * CH : (z + 1) * CH] = piece.astype(bf16)


def exchanged(x, axes):
    return lax.all_to_all(x, axes, split_axis=0, concat_axis=0, tiled=True)


def to_everyone(x, axes):
    copies = jnp.broadcast_to(x, (lax.axis_size(axes), *x.shape))
    return exchanged(copies, axes)


def shifted(x, axis):
    count = lax.axis_size(axis)
    pieces = []
    for steps in range(1, count):
        pieces.append(
            lax.ppermute(x, axis, [((k + steps) % count, k) for k in range(count)])
        )
    return pieces


def per_device(
    tokens,
    input_norm_gain,
    convolution_value_weight,
    convolution_gate_weight,
    depthwise_filter_taps,
    channel_norm_gain,
    channel_norm_bias,
    query_projection_weight,
    forget_gate_weight,
    recurrence_value_weight,
    output_gate_weight,
    forget_floor_margin,
    decay_jump_terms,
    head_norm_gain,
    convolution_output_weight,
    recurrence_output_weight,
):
    place = jnp.stack([lax.axis_index(a) for a in SP_TP]).astype(jnp.int32)
    width = tokens.shape[1]

    payload = kernel_call(prepare_body, shape((NC, 48, width), bf16), [VMEM] * 11)(
        tokens,
        input_norm_gain.reshape(1, width),
        query_projection_weight,
        forget_gate_weight,
        recurrence_value_weight,
        convolution_value_weight,
        convolution_gate_weight,
        output_gate_weight,
        convolution_output_weight,
        recurrence_output_weight,
        decay_jump_terms,
    )
    arrived = exchanged(payload, C)
    jumps = arrived[:, 40, : 2 * CH].astype(f32)
    jump = (jumps[:, :CH] + jumps[:, CH:]).reshape(1, ROWS)
    pair = arrived[:, 32:40]
    shard = jnp.concatenate([pair[:, :, :1024], pair[:, :, 1024:]], axis=1).reshape(32, 1024)
    own = arrived[:, :32].reshape(PAIR, width)
    rows = (own, *shifted(own, Y))

    out_along = to_everyone(shard[:, 768:], (ZH, ZL)).reshape(512, 256)
    along = lax.all_gather(shard[:, :768], (ZH, ZL), axis=0, tiled=True)
    rec_weight = to_everyone(along[:, :384], X).reshape(width, 384)
    conv_weight = to_everyone(along[:, 384:768], X).reshape(width, 384)

    margin = forget_floor_margin.reshape(1, 2 * CH)
    inner, decayed, packed = kernel_call(
        local_body,
        (shape((ROWS, CH), f32), shape((ROWS, CH), bf16), shape((STATE_ROWS, CH), bf16)),
        [SMEM] + [VMEM] * 7,
        [pltpu.VMEM((ROWS, 3 * CH), f32)],
    )(place, *rows, rec_weight, margin, jump)
    chips = lax.all_gather(packed, X, axis=0)

    def total_of(parts):
        return kernel_call(total_body, shape((STATE_ROWS, CH), bf16), [VMEM])(parts)

    slabs = to_everyone(total_of(chips), ZL)
    quads = to_everyone(total_of(slabs), ZH)

    out_pieces = (out_along, *shifted(out_along, X))

    value_gate, outgate, tail = kernel_call(
        project_body,
        (shape((ROWS, 2 * CH), bf16), shape((ROWS, CH), bf16), shape((HALO, 2 * CH), bf16)),
        [SMEM] + [VMEM] * 5,
        [pltpu.VMEM((ROWS, 3 * CH), f32)],
    )(place, *rows, conv_weight)
    blocks = NZ * NX
    halo = lax.ppermute(tail, (ZH, ZL, X), [(k, k + 1) for k in range(blocks - 1)])
    convolved, sums = kernel_call(
        conv_body,
        (shape((ROWS, CH), bf16), shape((8, ROWS), f32)),
        [SMEM, VMEM, VMEM, VMEM],
        [pltpu.VMEM((HALO + ROWS, CH), f32)],
    )(place, value_gate, halo, depthwise_filter_taps)
    all_sums = lax.all_gather(sums, (C, Y), axis=0)
    conv_out = kernel_call(channel_body, shape((ROWS, CH), bf16), [SMEM, VMEM, VMEM, VMEM, VMEM])(
        place,
        convolved,
        all_sums,
        channel_norm_gain.reshape(1, 2 * CH),
        channel_norm_bias.reshape(1, 2 * CH),
    )
    rec_out = kernel_call(
        finish_body, shape((ROWS, CH), bf16), [SMEM] + [VMEM] * 7
    )(place, quads, slabs, chips, inner, decayed, head_norm_gain.reshape(1, 2 * CH), outgate)

    partial = kernel_call(
        output_body, shape((NC, ROWS // NC, width), bf16), [SMEM] + [VMEM] * 6
    )(place, conv_out, rec_out, *out_pieces)
    pair_sum = exchanged(partial, C).astype(f32).sum(axis=0).astype(bf16)
    pieces = exchanged(pair_sum.reshape(NY, OWN, width), Y)
    return kernel_call(last_body, shape((OWN, width), bf16), [VMEM])(pieces)


def solution(mesh):
    split = Mesh(mesh.devices.reshape(NQ, NZ // NQ, NX, NC, mesh.shape["tp"]), SP_TP)
    return jax.shard_map(
        per_device,
        mesh=split,
        in_specs=(
            P(SP_TP, None),
            P(),
            P(SP, "tp"),
            P(SP, "tp"),
            P(None, "tp"),
            P("tp"),
            P("tp"),
            P(SP, "tp"),
            P(SP, "tp"),
            P(SP, "tp"),
            P(SP, "tp"),
            P("tp"),
            P("tp", SP),
            P("tp"),
            P("tp", SP),
            P("tp", SP),
        ),
        out_specs=P(SP_TP, None),
        check_vma=False,
    )
```

```python
import jax
import jax.numpy as jnp
from jax import lax
from jax.experimental import pallas as pl
from jax.experimental.pallas import tpu as pltpu
from jax.sharding import Mesh
from jax.sharding import PartitionSpec as P


ZH, ZL, X, C, Y = "sp_0", "sp_1", "sp_2", "sp_3", "tp"
SP = (ZH, ZL, X, C)
SP_TP = (ZH, ZL, X, C, Y)
NZ, NQ, NX, NC, NY = 16, 4, 4, 2, 4
CONV_CH = 1024
CH = 128
ROWS = 256
OWN = 32
BLOCK = 64
TAPS = 31
HALO = 32
STATE_ROWS = 136
HALF = 128
COLS = 384
CHUNK = 16
norm_eps = 1e-06
layer_eps = 1e-05
HIGH = lax.Precision.HIGHEST
bf16 = jnp.bfloat16
f32 = jnp.float32

VMEM = pl.BlockSpec(memory_space=pltpu.VMEM)
SMEM = pl.BlockSpec(memory_space=pltpu.SMEM)


def kernel_call(body, out, specs, scratch=()):
    return pl.pallas_call(
        body,
        out_shape=out,
        in_specs=specs,
        out_specs=jax.tree.map(lambda _: VMEM, out),
        scratch_shapes=scratch,
    )


def shape(dims, dtype):
    return jax.ShapeDtypeStruct(dims, dtype)


def matmul(a, b, dims, precision=None):
    return lax.dot_general(
        a, b, (dims, ((), ())), precision=precision, preferred_element_type=f32
    )


def sigmoid(v):
    return 1.0 / (1.0 + jnp.exp(-v))


def silu(v):
    return v * sigmoid(v)


def own_half(value, core):
    return jnp.where(core == 0, value[:, :CH], value[:, CH:])


def pack_body(query, forget, value, left, gate, outgate, conv_out, rec_out, out, rows):
    blocks = (query, forget, value, left, gate, outgate)
    for x in range(NX):
        mine = [3 * x + k for k in range(3)]
        for at, b in enumerate(sorted(mine, key=lambda b: ((b + x) % 2, b))):
            half = b % NC
            out[x, :, at * CH : (at + 1) * CH] = blocks[b // NC][:, half * CH : (half + 1) * CH]
    for c in range(NC):
        for k, block in enumerate((conv_out, rec_out)):
            at = (2 * c + k) * CH
            rows[:, at : at + CH] = block[:, c * CH : (c + 1) * CH]


def norm_body(tokens, gain, out):
    features = tokens[...].astype(f32)
    out[...] = (
        features
        * lax.rsqrt(jnp.mean(features * features, axis=1, keepdims=True) + norm_eps)
        * gain[...]
    ).astype(bf16)


def project_body(place, tokens, own, other, jump, out, weight):
    c = place[3]
    blocks = NZ * NX
    for core, piece in ((c, own), (1 - c, other)):

        def copy(k, carry, core=core, piece=piece):
            to = pl.multiple_of((NC * k + core) * CHUNK, CHUNK)
            weight[pl.ds(to, CHUNK)] = piece[pl.ds(pl.multiple_of(k * CHUNK, CHUNK), CHUNK)]
            return carry

        lax.fori_loop(0, blocks, copy, 0, unroll=8)
    even = lax.rem(place[2], 2)
    for x in range(NX):
        result = matmul(tokens[x * HALF : (x + 1) * HALF], weight[...], ((1,), (0,))).astype(bf16)
        first = NC * x + even
        second = NC * x + 1 - even
        out[first, :HALF] = result[:, : 2 * CH]
        out[second, :HALF, :CH] = result[:, 2 * CH :]
        out[second, :HALF, CH:] = jnp.zeros((HALF, CH), bf16)
        for k in range(NC):
            row = jnp.broadcast_to(jump[k : k + 1], (8, CH))
            high = row.astype(bf16)
            out[NC * x + k, HALF:, :CH] = high
            out[NC * x + k, HALF:, CH:] = (row - high.astype(f32)).astype(bf16)


PLACES = (
    ((0, 0), (0, 0)),
    ((0, 1), (1, 0)),
    ((1, 0), (1, 1)),
    ((2, 0), (2, 0)),
    ((2, 1), (3, 0)),
    ((3, 0), (3, 1)),
)


def block_of(spread, m, c):
    options = []
    for x, at in PLACES[m]:
        options.append(
            jnp.concatenate(
                [spread[NC * x + k, :HALF, at * CH : (at + 1) * CH] for k in range(NC)], axis=0
            )
        )
    if PLACES[m][0] == PLACES[m][1]:
        return options[0]
    return jnp.where(c == 0, options[0].astype(f32), options[1].astype(f32)).astype(bf16)


def local_body(place, spread, margin, inner, decayed, packed, tail):
    c = place[3]
    rows = []
    for k in range(NC):
        row = spread[NC * place[2] + k, HALF : HALF + 8].astype(f32)[:1]
        rows.append(row[:, :CH] + row[:, CH:])
    jump = jnp.concatenate(rows, axis=1)
    bound = own_half(margin[...], c)
    queries = silu(block_of(spread, 0, c).astype(f32))
    keys = bound * sigmoid(-block_of(spread, 1, c).astype(f32))
    inputs = block_of(spread, 2, c)
    for k in range(2):
        tail[:, k * CH : (k + 1) * CH] = block_of(spread, 3 + k, c)[ROWS - HALO :]
    log_forget = jnp.log1p(-keys)
    row = lax.broadcasted_iota(jnp.int32, (BLOCK, BLOCK), 0)
    col = lax.broadcasted_iota(jnp.int32, (BLOCK, BLOCK), 1)
    causal = row >= col
    lower = jnp.where(causal, 1.0, 0.0)
    state = jnp.zeros((CH, CH), f32)
    before = jnp.zeros((1, CH), f32)
    for n in range(ROWS // BLOCK):
        at = slice(n * BLOCK, (n + 1) * BLOCK)
        jumps = jump[:, n * BLOCK : (n + 1) * BLOCK]
        jumped = jnp.sum(jnp.where(causal, jumps, 0.0), axis=1, keepdims=True)
        running = matmul(lower, log_forget[at], ((1,), (0,)), HIGH) + jumped
        final = running[BLOCK - 1 : BLOCK]
        scaled = queries[at] * jnp.exp(running)
        scaled_keys = (keys[at] * jnp.exp(-running)).astype(bf16)
        final_keys = (keys[at] * jnp.exp(final - running)).astype(bf16)
        scores = matmul(scaled.astype(bf16), scaled_keys, ((1,), (1,)))
        scores = jnp.where(causal, scores, 0.0).astype(bf16)
        inner[at] = matmul(scores, inputs[at], ((1,), (0,))) + matmul(
            scaled.astype(bf16), state.astype(bf16), ((1,), (1,))
        )
        decayed[at] = (scaled * jnp.exp(before)).astype(bf16)
        state = state * jnp.exp(final) + matmul(inputs[at], final_keys, ((0,), (0,)))
        before = before + final
    pack(packed, state, before)


def pack(ref, state, decay):
    high = decay.astype(bf16).astype(f32)
    low = decay - high
    first = lax.broadcasted_iota(jnp.int32, (8, CH), 0)
    ref[:CH] = state.astype(bf16)
    ref[CH:] = jnp.where(first == 0, high, jnp.where(first == 1, low, 0.0)).astype(bf16)


def unpacked(block):
    wide = block.astype(f32)
    return wide[CH : CH + 1] + wide[CH + 1 : CH + 2], wide[:CH]


def total_body(parts, total):
    state = jnp.zeros((CH, CH), f32)
    decay = jnp.zeros((1, CH), f32)
    for k in range(NQ):
        step, add = unpacked(parts[k])
        state = state * jnp.exp(step) + add
        decay = decay + step
    for k in range(total.shape[0]):
        pack(total.at[k], state, decay)


def finish_body(place, quads, slabs, chips, inner, decayed, gain, spread, out):
    state = jnp.zeros((CH, CH), f32)
    for level, parts in enumerate((quads, slabs, chips)):
        for k in range(NQ):
            step, add = unpacked(parts[k])
            state = jnp.where(k < place[level], state * jnp.exp(step) + add, state)
    recurrent = inner[...] + matmul(decayed[...], state.astype(bf16), ((1,), (1,)))
    scale = lax.rsqrt(jnp.mean(recurrent * recurrent, axis=1, keepdims=True) + norm_eps)
    gate = silu(block_of(spread, 5, place[3]).astype(f32))
    out[...] = (recurrent * scale * own_half(gain[...], place[3]) * gate).astype(bf16)


def conv_body(place, spread, halo, taps, out, sums, gated):
    rim = halo[...].astype(f32)
    gated[:HALO] = rim[:, :CH] * sigmoid(rim[:, CH:])
    c = place[3]
    gated[HALO:] = block_of(spread, 3, c).astype(f32) * sigmoid(block_of(spread, 4, c).astype(f32))
    own_taps = own_half(taps[...], place[3])
    for n in range(ROWS // BLOCK):
        total = jnp.zeros((BLOCK, CH), f32)
        for j in range(TAPS):
            at = n * BLOCK + HALO - TAPS + 1 + j
            total = total + gated[at : at + BLOCK] * own_taps[j : j + 1]
        out[n * BLOCK : (n + 1) * BLOCK] = total.astype(bf16)
    values = out[...].astype(f32)
    ones = jnp.ones((8, CH), f32)
    first_sum = matmul(ones, values, ((1,), (1,)), HIGH)
    second_sum = matmul(ones, values * values, ((1,), (1,)), HIGH)
    row = lax.broadcasted_iota(jnp.int32, (8, ROWS), 0)
    both_sums = jnp.where(row == 0, first_sum, second_sum)
    for k in range(NC * NY):
        sums[k] = both_sums


def channel_body(place, values, sums, gain, bias, out):
    total = sums[0]
    for k in range(1, NC * NY):
        total = total + sums[k]
    row = lax.broadcasted_iota(jnp.int32, (8, CH), 0)
    pick_first = jnp.where(row == 0, 1.0 / CONV_CH, 0.0)
    pick_second = jnp.where(row == 1, 1.0 / CONV_CH, 0.0)
    mean = matmul(total, pick_first, ((0,), (0,)), HIGH)
    variance = matmul(total, pick_second, ((0,), (0,)), HIGH) - mean * mean
    shifted = (values[...].astype(f32) - mean) * lax.rsqrt(variance + layer_eps)
    out[...] = silu(
        shifted * own_half(gain[...], place[3]) + own_half(bias[...], place[3])
    ).astype(bf16)


def output_body(conv_out, rec_out, pieces, out, weight):
    for k in range(NX * NC):
        for z in range(NZ):
            to = (z * NX * NC + k) * CHUNK
            weight[to : to + CHUNK] = pieces[k, z * CHUNK : (z + 1) * CHUNK]
    both = jnp.concatenate([conv_out[...], rec_out[...]], axis=1)
    result = matmul(both, weight[...], ((1,), (1,))).astype(bf16)
    for c in range(NC):
        out[c] = result[c * HALF : (c + 1) * HALF]


def last_body(parts, out):
    total = parts[0].astype(f32)
    for y in range(1, NY):
        total = total + parts[y].astype(f32)
    out[...] = total.astype(bf16)


def exchanged(x, axes):
    return lax.all_to_all(x, axes, split_axis=0, concat_axis=0, tiled=True)


def to_everyone(x, axes):
    copies = jnp.broadcast_to(x, (lax.axis_size(axes), *x.shape))
    return exchanged(copies, axes)


def per_device(
    tokens,
    input_norm_gain,
    convolution_value_weight,
    convolution_gate_weight,
    depthwise_filter_taps,
    channel_norm_gain,
    channel_norm_bias,
    query_projection_weight,
    forget_gate_weight,
    recurrence_value_weight,
    output_gate_weight,
    forget_floor_margin,
    decay_jump_terms,
    head_norm_gain,
    convolution_output_weight,
    recurrence_output_weight,
):
    place = jnp.stack([lax.axis_index(a) for a in SP_TP]).astype(jnp.int32)
    width = tokens.shape[1]

    columns, out_rows = kernel_call(
        pack_body, (shape((NX, CHUNK, COLS), bf16), shape((CHUNK, 4 * CH), bf16)), [VMEM] * 8
    )(
        query_projection_weight,
        forget_gate_weight,
        recurrence_value_weight,
        convolution_value_weight,
        convolution_gate_weight,
        output_gate_weight,
        convolution_output_weight.T,
        recurrence_output_weight.T,
    )
    shard = exchanged(columns, X).reshape(NX * CHUNK, COLS)
    normed = kernel_call(norm_body, shape((OWN, width), bf16), [VMEM, VMEM])(
        tokens, input_norm_gain.reshape(1, width)
    )
    rows = to_everyone(normed, (X, Y)).reshape(NX * HALF, width)
    own = lax.all_gather(shard, (ZH, ZL), axis=0, tiled=True)
    other = lax.ppermute(own, C, [(0, 1), (1, 0)])
    spread = kernel_call(
        project_body,
        shape((NX * NC, HALF + 8, 2 * CH), bf16),
        [SMEM] + [VMEM] * 4,
        [pltpu.VMEM((width, COLS), bf16)],
    )(place, rows, own, other, decay_jump_terms)
    spread = exchanged(spread, (X, C))
    out_along = to_everyone(out_rows, (ZH, ZL))
    halves = out_along.reshape(NZ * CHUNK, NC, 2 * CH).transpose(1, 0, 2)
    halves = jnp.broadcast_to(halves, (NX, *halves.shape)).reshape(-1, *halves.shape[1:])
    out_pieces = exchanged(halves, (X, C))

    margin = forget_floor_margin.reshape(1, 2 * CH)
    inner, decayed, packed, tail = kernel_call(
        local_body,
        (
            shape((ROWS, CH), f32),
            shape((ROWS, CH), bf16),
            shape((STATE_ROWS, CH), bf16),
            shape((HALO, 2 * CH), bf16),
        ),
        [SMEM] + [VMEM] * 2,
    )(place, spread, margin)
    chips = lax.all_gather(packed, X, axis=0)

    def total_of(parts, copies):
        return kernel_call(total_body, shape((copies, STATE_ROWS, CH), bf16), [VMEM])(parts)

    slab_copies = total_of(chips, NQ)
    slabs = exchanged(slab_copies, ZL)
    quad = total_of(slabs, 1)[0]
    quads = lax.all_gather(quad, ZH, axis=0)

    blocks = NZ * NX
    halo = lax.ppermute(tail, (ZH, ZL, X), [(k, k + 1) for k in range(blocks - 1)])
    convolved, sums = kernel_call(
        conv_body,
        (shape((ROWS, CH), bf16), shape((NC * NY, 8, ROWS), f32)),
        [SMEM, VMEM, VMEM, VMEM],
        [pltpu.VMEM((HALO + ROWS, CH), f32)],
    )(place, spread, halo, depthwise_filter_taps)
    all_sums = exchanged(sums, (C, Y))
    conv_out = kernel_call(channel_body, shape((ROWS, CH), bf16), [SMEM, VMEM, VMEM, VMEM, VMEM])(
        place,
        convolved,
        all_sums,
        channel_norm_gain.reshape(1, 2 * CH),
        channel_norm_bias.reshape(1, 2 * CH),
    )
    rec_out = kernel_call(
        finish_body, shape((ROWS, CH), bf16), [SMEM] + [VMEM] * 7
    )(place, quads, slabs, chips, inner, decayed, head_norm_gain.reshape(1, 2 * CH), spread)

    partial = kernel_call(
        output_body, shape((NC, ROWS // NC, width), bf16), [VMEM] * 3,
        [pltpu.VMEM((width, 2 * CH), bf16)],
    )(conv_out, rec_out, out_pieces)
    pair_sum = exchanged(partial, C).astype(f32).sum(axis=0).astype(bf16)
    pieces = exchanged(pair_sum.reshape(NY, OWN, width), Y)
    return kernel_call(last_body, shape((OWN, width), bf16), [VMEM])(pieces)


def solution(mesh):
    split = Mesh(mesh.devices.reshape(NQ, NZ // NQ, NX, NC, mesh.shape["tp"]), SP_TP)
    return jax.shard_map(
        per_device,
        mesh=split,
        in_specs=(
            P(SP_TP, None),
            P(),
            P(SP, "tp"),
            P(SP, "tp"),
            P(None, "tp"),
            P("tp"),
            P("tp"),
            P(SP, "tp"),
            P(SP, "tp"),
            P(SP, "tp"),
            P(SP, "tp"),
            P("tp"),
            P("tp", SP),
            P("tp"),
            P("tp", SP),
            P("tp", SP),
        ),
        out_specs=P(SP_TP, None),
        check_vma=False,
    )
```

```python
import jax
import jax.numpy as jnp
from jax import lax
from jax.experimental import pallas as pl
from jax.experimental.pallas import tpu as pltpu
from jax.sharding import Mesh
from jax.sharding import PartitionSpec as P


ZH, ZL, X, C, Y = "sp_0", "sp_1", "sp_2", "sp_3", "tp"
SP = (ZH, ZL, X, C)
SP_TP = (ZH, ZL, X, C, Y)
NZ, NQ, NX, NC, NY = 16, 4, 4, 2, 4
CONV_CH = 1024
CH = 128
ROWS = 256
OWN = 32
BLOCK = 64
TAPS = 31
HALO = 32
STATE_ROWS = 136
HALF = 128
CHUNK = 16
COLUMN_ROWS = 24
OUT_ROWS = 32
SENT_ROWS = 64
norm_eps = 1e-06
layer_eps = 1e-05
HIGH = lax.Precision.HIGHEST
bf16 = jnp.bfloat16
f32 = jnp.float32

VMEM = pl.BlockSpec(memory_space=pltpu.VMEM)
SMEM = pl.BlockSpec(memory_space=pltpu.SMEM)


def kernel_call(body, out, specs, scratch=()):
    return pl.pallas_call(
        body,
        out_shape=out,
        in_specs=specs,
        out_specs=jax.tree.map(lambda _: VMEM, out),
        scratch_shapes=scratch,
    )


def shape(dims, dtype):
    return jax.ShapeDtypeStruct(dims, dtype)


def matmul(a, b, dims, precision=None):
    return lax.dot_general(
        a, b, (dims, ((), ())), precision=precision, preferred_element_type=f32
    )


def sigmoid(v):
    return 1.0 / (1.0 + jnp.exp(-v))


def silu(v):
    return v * sigmoid(v)


def own_half(value, core):
    return jnp.where(core == 0, value[:, :CH], value[:, CH:])


def pack_body(query, forget, value, left, gate, outgate, conv_out, rec_out, jump, out):
    whole = (query, value, left, outgate)
    split = (forget, forget, gate, gate)
    lane = lax.broadcasted_iota(jnp.int32, (8, CH), 1)
    for c in range(NC):
        half = slice(c * CH, (c + 1) * CH)
        row = jnp.broadcast_to(jump[c : c + 1], (8, CH))
        high = row.astype(bf16).astype(f32)
        first = lax.broadcasted_iota(jnp.int32, (8, CH), 0)
        jumps = jnp.where(first == 0, high, row - high).astype(bf16)
        for x in range(NX):
            to = NC * x + c
            out[to, :CHUNK] = whole[x][:, half]
            rows = split[x][:, half].astype(f32)
            turned = pltpu.roll(rows[8:], CH // 2, 1)
            keep = lane < CH // 2 if x % 2 == 0 else lane >= CH // 2
            out[to, CHUNK:COLUMN_ROWS] = jnp.where(keep, rows[:8], turned).astype(bf16)
            out[to, COLUMN_ROWS : COLUMN_ROWS + CHUNK] = conv_out[:, half]
            out[to, COLUMN_ROWS + CHUNK : COLUMN_ROWS + OUT_ROWS] = rec_out[:, half]
            out[to, COLUMN_ROWS + OUT_ROWS :] = jumps


def norm_body(tokens, gain, out):
    features = tokens[...].astype(f32)
    normed = (
        features
        * lax.rsqrt(jnp.mean(features * features, axis=1, keepdims=True) + norm_eps)
        * gain[...]
    ).astype(bf16)
    for k in range(NX * NY):
        out[k] = normed


def project_body(place, own, other, columns, out, weight):
    c = place[3]
    blocks = NX * NC
    step = blocks * CHUNK
    for z in range(NZ):
        at = z * step
        piece = columns[z * blocks : (z + 1) * blocks]
        weight[at : at + step, :CH] = piece[:, :CHUNK].reshape(step, CH)
        packed = piece[:, CHUNK:].reshape(blocks * 8, CH).astype(f32)
        turned = pltpu.roll(packed, CH // 2, 1).reshape(blocks, 8, CH)
        both = jnp.concatenate([packed.reshape(blocks, 8, CH), turned], axis=1)
        weight[at : at + step, CH:] = both.reshape(step, CH).astype(bf16)
    for k in range(NX):
        x = lax.rem(place[2] + k, NX)
        rows = pl.ds(pl.multiple_of(x * HALF, HALF), HALF)
        for core, tokens in ((c, own), (1 - c, other)):
            to = pl.ds(pl.multiple_of(core * HALF, HALF), HALF)
            out[k, to] = matmul(tokens[rows], weight[...], ((1,), (0,))).astype(bf16)


def source(pieces, place, x, second):
    slot = lax.rem(place[2] - x + NX, NX)
    at = slice(CH, 2 * CH) if second else slice(0, CH)
    value = pieces[0][:, at].astype(f32)
    for k in range(1, NX):
        value = jnp.where(slot == k, pieces[k][:, at].astype(f32), value)
    return value


def joined(pieces, place, x):
    lane = lax.broadcasted_iota(jnp.int32, (ROWS, CH), 1)
    return jnp.where(
        lane < CH // 2, source(pieces, place, x, True), source(pieces, place, x + 1, True)
    )


def local_body(place, p0, p1, p2, p3, margin, jumps, inner, decayed, packed, rest, tail):
    c = place[3]
    pieces = (p0, p1, p2, p3)
    jump = jnp.concatenate(
        [
            jumps[k, :1].astype(f32) + jumps[k, 1:2].astype(f32)
            for k in range(NC)
        ],
        axis=1,
    )
    bound = own_half(margin[...], c)
    queries = silu(source(pieces, place, 0, False))
    keys = bound * sigmoid(-joined(pieces, place, 0))
    inputs = source(pieces, place, 1, False).astype(bf16)
    others = (
        source(pieces, place, 2, False),
        joined(pieces, place, 2),
        source(pieces, place, 3, False),
    )
    for k, value in enumerate(others):
        rest[:, k * CH : (k + 1) * CH] = value.astype(bf16)
        if k < 2:
            tail[:, k * CH : (k + 1) * CH] = value[ROWS - HALO :].astype(bf16)
    log_forget = jnp.log1p(-keys)
    row = lax.broadcasted_iota(jnp.int32, (BLOCK, BLOCK), 0)
    col = lax.broadcasted_iota(jnp.int32, (BLOCK, BLOCK), 1)
    causal = row >= col
    lower = jnp.where(causal, 1.0, 0.0)
    state = jnp.zeros((CH, CH), f32)
    before = jnp.zeros((1, CH), f32)
    for n in range(ROWS // BLOCK):
        at = slice(n * BLOCK, (n + 1) * BLOCK)
        jumps = jump[:, n * BLOCK : (n + 1) * BLOCK]
        jumped = jnp.sum(jnp.where(causal, jumps, 0.0), axis=1, keepdims=True)
        running = matmul(lower, log_forget[at], ((1,), (0,)), HIGH) + jumped
        final = running[BLOCK - 1 : BLOCK]
        scaled = queries[at] * jnp.exp(running)
        scaled_keys = (keys[at] * jnp.exp(-running)).astype(bf16)
        final_keys = (keys[at] * jnp.exp(final - running)).astype(bf16)
        scores = matmul(scaled.astype(bf16), scaled_keys, ((1,), (1,)))
        scores = jnp.where(causal, scores, 0.0).astype(bf16)
        inner[at] = matmul(scores, inputs[at], ((1,), (0,))) + matmul(
            scaled.astype(bf16), state.astype(bf16), ((1,), (1,))
        )
        decayed[at] = (scaled * jnp.exp(before)).astype(bf16)
        state = state * jnp.exp(final) + matmul(inputs[at], final_keys, ((0,), (0,)))
        before = before + final
    pack(packed, state, before)


def pack(ref, state, decay):
    high = decay.astype(bf16).astype(f32)
    low = decay - high
    first = lax.broadcasted_iota(jnp.int32, (8, CH), 0)
    ref[:CH] = state.astype(bf16)
    ref[CH:] = jnp.where(first == 0, high, jnp.where(first == 1, low, 0.0)).astype(bf16)


def unpacked(block):
    wide = block.astype(f32)
    return wide[CH : CH + 1] + wide[CH + 1 : CH + 2], wide[:CH]


def total_body(parts, total):
    state = jnp.zeros((CH, CH), f32)
    decay = jnp.zeros((1, CH), f32)
    for k in range(NQ):
        step, add = unpacked(parts[k])
        state = state * jnp.exp(step) + add
        decay = decay + step
    for k in range(total.shape[0]):
        pack(total.at[k], state, decay)


def finish_body(place, quads, slabs, chips, inner, decayed, gain, rest, out):
    state = jnp.zeros((CH, CH), f32)
    for level, parts in enumerate((quads, slabs, chips)):
        for k in range(NQ):
            step, add = unpacked(parts[k])
            state = jnp.where(k < place[level], state * jnp.exp(step) + add, state)
    recurrent = inner[...] + matmul(decayed[...], state.astype(bf16), ((1,), (1,)))
    scale = lax.rsqrt(jnp.mean(recurrent * recurrent, axis=1, keepdims=True) + norm_eps)
    gate = silu(rest[:, 2 * CH :].astype(f32))
    out[...] = (recurrent * scale * own_half(gain[...], place[3]) * gate).astype(bf16)


def conv_body(place, rest, halo, taps, out, sums, gated):
    rim = halo[...].astype(f32)
    gated[:HALO] = rim[:, :CH] * sigmoid(rim[:, CH:])
    gated[HALO:] = rest[:, :CH].astype(f32) * sigmoid(rest[:, CH : 2 * CH].astype(f32))
    own_taps = own_half(taps[...], place[3])
    for n in range(ROWS // BLOCK):
        total = jnp.zeros((BLOCK, CH), f32)
        for j in range(TAPS):
            at = n * BLOCK + HALO - TAPS + 1 + j
            total = total + gated[at : at + BLOCK] * own_taps[j : j + 1]
        out[n * BLOCK : (n + 1) * BLOCK] = total.astype(bf16)
    values = out[...].astype(f32)
    ones = jnp.ones((8, CH), f32)
    first_sum = matmul(ones, values, ((1,), (1,)), HIGH)
    second_sum = matmul(ones, values * values, ((1,), (1,)), HIGH)
    row = lax.broadcasted_iota(jnp.int32, (8, ROWS), 0)
    both_sums = jnp.where(row == 0, first_sum, second_sum)
    for k in range(NC * NY):
        sums[k] = both_sums


def channel_body(place, values, sums, gain, bias, out):
    total = sums[0]
    for k in range(1, NC * NY):
        total = total + sums[k]
    row = lax.broadcasted_iota(jnp.int32, (8, CH), 0)
    pick_first = jnp.where(row == 0, 1.0 / CONV_CH, 0.0)
    pick_second = jnp.where(row == 1, 1.0 / CONV_CH, 0.0)
    mean = matmul(total, pick_first, ((0,), (0,)), HIGH)
    variance = matmul(total, pick_second, ((0,), (0,)), HIGH) - mean * mean
    shifted = (values[...].astype(f32) - mean) * lax.rsqrt(variance + layer_eps)
    out[...] = silu(
        shifted * own_half(gain[...], place[3]) + own_half(bias[...], place[3])
    ).astype(bf16)


def output_body(place, conv_out, rec_out, pieces, mine, theirs, weight, both):
    blocks = NX * NC
    step = blocks * CHUNK
    for z in range(NZ):
        at = z * step
        piece = pieces[z]
        weight[at : at + step, :CH] = piece[:, :CHUNK].reshape(step, CH)
        weight[at : at + step, CH:] = piece[:, CHUNK:].reshape(step, CH)
    both[:, :CH] = conv_out[...]
    both[:, CH:] = rec_out[...]
    for core, out in ((place[3], mine), (1 - place[3], theirs)):
        rows = pl.ds(pl.multiple_of(core * HALF, HALF), HALF)
        out[...] = matmul(both[rows], weight[...], ((1,), (1,))).astype(bf16)


def last_body(parts, out):
    total = parts[0].astype(f32)
    for y in range(1, NY):
        total = total + parts[y].astype(f32)
    out[...] = total.astype(bf16)


def exchanged(x, axes):
    return lax.all_to_all(x, axes, split_axis=0, concat_axis=0, tiled=True)


def to_everyone(x, axes):
    copies = jnp.broadcast_to(x, (lax.axis_size(axes), *x.shape))
    return exchanged(copies, axes)


def per_device(
    tokens,
    input_norm_gain,
    convolution_value_weight,
    convolution_gate_weight,
    depthwise_filter_taps,
    channel_norm_gain,
    channel_norm_bias,
    query_projection_weight,
    forget_gate_weight,
    recurrence_value_weight,
    output_gate_weight,
    forget_floor_margin,
    decay_jump_terms,
    head_norm_gain,
    convolution_output_weight,
    recurrence_output_weight,
):
    place = jnp.stack([lax.axis_index(a) for a in SP_TP]).astype(jnp.int32)
    width = tokens.shape[1]

    payload = kernel_call(pack_body, shape((NX * NC, SENT_ROWS, CH), bf16), [VMEM] * 9)(
        query_projection_weight,
        forget_gate_weight,
        recurrence_value_weight,
        convolution_value_weight,
        convolution_gate_weight,
        output_gate_weight,
        convolution_output_weight.T,
        recurrence_output_weight.T,
        decay_jump_terms,
    )
    arrived = exchanged(payload, (X, C))
    copies = kernel_call(
        norm_body, shape((NX * NY, OWN, width), bf16), [VMEM, VMEM]
    )(tokens, input_norm_gain.reshape(1, width))
    own = exchanged(copies, (X, Y)).reshape(NX * HALF, width)
    other = lax.ppermute(own, C, [(0, 1), (1, 0)])
    columns = lax.all_gather(arrived[:, :COLUMN_ROWS], (ZH, ZL), axis=0, tiled=True)
    out_pieces = to_everyone(arrived[:, COLUMN_ROWS : COLUMN_ROWS + OUT_ROWS], (ZH, ZL))
    jumps = lax.dynamic_slice_in_dim(
        arrived[:, COLUMN_ROWS + OUT_ROWS :], NC * lax.axis_index(X), NC, axis=0
    )
    projected = kernel_call(
        project_body,
        shape((NX, ROWS, 2 * CH), bf16),
        [SMEM] + [VMEM] * 3,
        [pltpu.VMEM((width, 2 * CH), bf16)],
    )(place, own, other, columns)
    pieces = [projected[0]]
    for k in range(1, NX):
        pieces.append(
            lax.ppermute(projected[k], X, [(x, (x + k) % NX) for x in range(NX)])
        )

    margin = forget_floor_margin.reshape(1, 2 * CH)
    inner, decayed, packed, rest, tail = kernel_call(
        local_body,
        (
            shape((ROWS, CH), f32),
            shape((ROWS, CH), bf16),
            shape((STATE_ROWS, CH), bf16),
            shape((ROWS, 3 * CH), bf16),
            shape((HALO, 2 * CH), bf16),
        ),
        [SMEM] + [VMEM] * 6,
    )(place, *pieces, margin, jumps)
    chips = lax.all_gather(packed, X, axis=0)

    def total_of(parts, copies):
        return kernel_call(
            total_body, shape((copies, STATE_ROWS, CH), bf16), [VMEM]
        )(parts)

    slab_copies = total_of(chips, NQ)
    slabs = exchanged(slab_copies, ZL)
    quad_copies = total_of(slabs, NQ)
    quads = exchanged(quad_copies, ZH)

    blocks = NZ * NX
    halo = lax.ppermute(tail, (ZH, ZL, X), [(k, k + 1) for k in range(blocks - 1)])
    convolved, sums = kernel_call(
        conv_body,
        (shape((ROWS, CH), bf16), shape((NC * NY, 8, ROWS), f32)),
        [SMEM, VMEM, VMEM, VMEM],
        [pltpu.VMEM((HALO + ROWS, CH), f32)],
    )(place, rest, halo, depthwise_filter_taps)
    all_sums = exchanged(sums, (C, Y))
    conv_out = kernel_call(
        channel_body, shape((ROWS, CH), bf16), [SMEM, VMEM, VMEM, VMEM, VMEM]
    )(
        place,
        convolved,
        all_sums,
        channel_norm_gain.reshape(1, 2 * CH),
        channel_norm_bias.reshape(1, 2 * CH),
    )
    rec_out = kernel_call(
        finish_body, shape((ROWS, CH), bf16), [SMEM] + [VMEM] * 7
    )(place, quads, slabs, chips, inner, decayed, head_norm_gain.reshape(1, 2 * CH), rest)

    mine, theirs = kernel_call(
        output_body,
        (shape((HALF, width), bf16), shape((HALF, width), bf16)),
        [SMEM] + [VMEM] * 3,
        [pltpu.VMEM((width, 2 * CH), bf16), pltpu.VMEM((ROWS, 2 * CH), bf16)],
    )(place, conv_out, rec_out, out_pieces)
    given = lax.ppermute(theirs, C, [(0, 1), (1, 0)])
    pair_sum = (mine.astype(f32) + given.astype(f32)).astype(bf16)
    pieces = exchanged(pair_sum.reshape(NY, OWN, width), Y)
    return kernel_call(last_body, shape((OWN, width), bf16), [VMEM])(pieces)


def solution(mesh):
    split = Mesh(mesh.devices.reshape(NQ, NZ // NQ, NX, NC, mesh.shape["tp"]), SP_TP)
    return jax.shard_map(
        per_device,
        mesh=split,
        in_specs=(
            P(SP_TP, None),
            P(),
            P(SP, "tp"),
            P(SP, "tp"),
            P(None, "tp"),
            P("tp"),
            P("tp"),
            P(SP, "tp"),
            P(SP, "tp"),
            P(SP, "tp"),
            P(SP, "tp"),
            P("tp"),
            P("tp", SP),
            P("tp"),
            P("tp", SP),
            P("tp", SP),
        ),
        out_specs=P(SP_TP, None),
        check_vma=False,
    )
```

```python
import jax
import jax.numpy as jnp
from jax import lax
from jax.experimental import pallas as pl
from jax.experimental.pallas import tpu as pltpu
from jax.sharding import Mesh
from jax.sharding import PartitionSpec as P


ZH, ZL, X, C, Y = "sp_0", "sp_1", "sp_2", "sp_3", "tp"
SP = (ZH, ZL, X, C)
SP_TP = (ZH, ZL, X, C, Y)
NZ, NQ, NX, NC, NY = 16, 4, 4, 2, 4
CONV_CH = 1024
CH = 128
ROWS = 256
OWN = 32
BLOCK = 64
TAPS = 31
HALO = 32
STATE_ROWS = 136
HALF = 128
CHUNK = 16
COLUMN_ROWS = 24
OUT_ROWS = 32
SENT_ROWS = 64
CARRIED = 7
norm_eps = 1e-06
layer_eps = 1e-05
HIGH = lax.Precision.HIGHEST
bf16 = jnp.bfloat16
f32 = jnp.float32

VMEM = pl.BlockSpec(memory_space=pltpu.VMEM)
SMEM = pl.BlockSpec(memory_space=pltpu.SMEM)


def kernel_call(body, out, specs, scratch=()):
    return pl.pallas_call(
        body,
        out_shape=out,
        in_specs=specs,
        out_specs=jax.tree.map(lambda _: VMEM, out),
        scratch_shapes=scratch,
    )


def shape(dims, dtype):
    return jax.ShapeDtypeStruct(dims, dtype)


def matmul(a, b, dims, precision=None):
    return lax.dot_general(
        a, b, (dims, ((), ())), precision=precision, preferred_element_type=f32
    )


def sigmoid(v):
    return 1.0 / (1.0 + jnp.exp(-v))


def silu(v):
    return v * sigmoid(v)


def own_half(value, core):
    return jnp.where(core == 0, value[:, :CH], value[:, CH:])


def pack_body(query, forget, value, left, gate, outgate, conv_out, rec_out, jump, out):
    whole = (query, value, left, outgate)
    split = (forget, forget, gate, gate)
    lane = lax.broadcasted_iota(jnp.int32, (8, CH), 1)
    for c in range(NC):
        half = slice(c * CH, (c + 1) * CH)
        row = jnp.broadcast_to(jump[c : c + 1], (8, CH))
        high = row.astype(bf16).astype(f32)
        first = lax.broadcasted_iota(jnp.int32, (8, CH), 0)
        jumps = jnp.where(first == 0, high, row - high).astype(bf16)
        for x in range(NX):
            to = NC * x + c
            out[to, :CHUNK] = whole[x][:, half]
            rows = split[x][:, half].astype(f32)
            turned = pltpu.roll(rows[8:], CH // 2, 1)
            keep = lane < CH // 2 if x % 2 == 0 else lane >= CH // 2
            out[to, CHUNK:COLUMN_ROWS] = jnp.where(keep, rows[:8], turned).astype(bf16)
            out[to, COLUMN_ROWS : COLUMN_ROWS + CHUNK] = conv_out[:, half]
            out[to, COLUMN_ROWS + CHUNK : COLUMN_ROWS + OUT_ROWS] = rec_out[:, half]
            out[to, COLUMN_ROWS + OUT_ROWS :] = jumps


def norm_body(tokens, gain, out):
    features = tokens[...].astype(f32)
    normed = (
        features
        * lax.rsqrt(jnp.mean(features * features, axis=1, keepdims=True) + norm_eps)
        * gain[...]
    ).astype(bf16)
    for k in range(NX * NY):
        out[k] = normed


def sort_body(arrived, along, rest):
    blocks = NX * NC
    split = COLUMN_ROWS + OUT_ROWS - 8
    for k in range(blocks):
        along[k * COLUMN_ROWS : (k + 1) * COLUMN_ROWS] = arrived[k, :COLUMN_ROWS]
        rest[k * 24 : (k + 1) * 24] = arrived[k, COLUMN_ROWS:split]
        last = arrived[k, split : split + 8]
        if k < CARRIED:
            at = blocks * COLUMN_ROWS + k * 8
            along[at : at + 8] = last
        else:
            rest[blocks * 24 :] = last


def project_body(place, own, other, columns, out0, out1, out2, out3, weight):
    c = place[3]
    blocks = NX * NC
    step = blocks * CHUNK
    for z in range(NZ):
        at = z * step
        piece = columns[z, : blocks * COLUMN_ROWS].reshape(blocks, COLUMN_ROWS, CH)
        weight[at : at + step, :CH] = piece[:, :CHUNK].reshape(step, CH)
        packed = piece[:, CHUNK:].reshape(blocks * 8, CH).astype(f32)
        turned = pltpu.roll(packed, CH // 2, 1).reshape(blocks, 8, CH)
        both = jnp.concatenate([packed.reshape(blocks, 8, CH), turned], axis=1)
        weight[at : at + step, CH:] = both.reshape(step, CH).astype(bf16)
    outs = (out0, out1, out2, out3)
    for k in range(NX):
        x = lax.rem(place[2] + k, NX)
        rows = pl.ds(pl.multiple_of(x * HALF, HALF), HALF)
        for core, tokens in ((c, own), (1 - c, other)):
            to = pl.ds(pl.multiple_of(core * HALF, HALF), HALF)
            outs[k][to] = matmul(tokens[rows], weight[...], ((1,), (0,))).astype(bf16)


def source(pieces, place, x, second):
    slot = lax.rem(place[2] - x + NX, NX)
    at = slice(CH, 2 * CH) if second else slice(0, CH)
    value = pieces[0][:, at].astype(f32)
    for k in range(1, NX):
        value = jnp.where(slot == k, pieces[k][:, at].astype(f32), value)
    return value


def joined(pieces, place, x):
    lane = lax.broadcasted_iota(jnp.int32, (ROWS, CH), 1)
    return jnp.where(
        lane < CH // 2, source(pieces, place, x, True), source(pieces, place, x + 1, True)
    )


def local_body(place, p0, p1, p2, p3, margin, arrived, inner, decayed, packed, rest, tail):
    c = place[3]
    pieces = (p0, p1, p2, p3)
    at = COLUMN_ROWS + OUT_ROWS
    rows = [arrived[NC * place[2] + k, at : at + 8].astype(f32) for k in range(NC)]
    jump = jnp.concatenate([r[:1] + r[1:2] for r in rows], axis=1)
    bound = own_half(margin[...], c)
    queries = silu(source(pieces, place, 0, False))
    keys = bound * sigmoid(-joined(pieces, place, 0))
    inputs = source(pieces, place, 1, False).astype(bf16)
    others = (
        source(pieces, place, 2, False),
        joined(pieces, place, 2),
        source(pieces, place, 3, False),
    )
    for k, value in enumerate(others):
        rest[:, k * CH : (k + 1) * CH] = value.astype(bf16)
        if k < 2:
            tail[:, k * CH : (k + 1) * CH] = value[ROWS - HALO :].astype(bf16)
    log_forget = jnp.log1p(-keys)
    row = lax.broadcasted_iota(jnp.int32, (BLOCK, BLOCK), 0)
    col = lax.broadcasted_iota(jnp.int32, (BLOCK, BLOCK), 1)
    causal = row >= col
    lower = jnp.where(causal, 1.0, 0.0)
    state = jnp.zeros((CH, CH), f32)
    before = jnp.zeros((1, CH), f32)
    for n in range(ROWS // BLOCK):
        at = slice(n * BLOCK, (n + 1) * BLOCK)
        jumps = jump[:, n * BLOCK : (n + 1) * BLOCK]
        jumped = jnp.sum(jnp.where(causal, jumps, 0.0), axis=1, keepdims=True)
        running = matmul(lower, log_forget[at], ((1,), (0,)), HIGH) + jumped
        final = running[BLOCK - 1 : BLOCK]
        scaled = queries[at] * jnp.exp(running)
        scaled_keys = (keys[at] * jnp.exp(-running)).astype(bf16)
        final_keys = (keys[at] * jnp.exp(final - running)).astype(bf16)
        scores = matmul(scaled.astype(bf16), scaled_keys, ((1,), (1,)))
        scores = jnp.where(causal, scores, 0.0).astype(bf16)
        inner[at] = matmul(scores, inputs[at], ((1,), (0,))) + matmul(
            scaled.astype(bf16), state.astype(bf16), ((1,), (1,))
        )
        decayed[at] = (scaled * jnp.exp(before)).astype(bf16)
        state = state * jnp.exp(final) + matmul(inputs[at], final_keys, ((0,), (0,)))
        before = before + final
    pack(packed, state, before)


def pack(ref, state, decay):
    high = decay.astype(bf16).astype(f32)
    low = decay - high
    first = lax.broadcasted_iota(jnp.int32, (8, CH), 0)
    ref[:CH] = state.astype(bf16)
    ref[CH:] = jnp.where(first == 0, high, jnp.where(first == 1, low, 0.0)).astype(bf16)


def unpacked(block):
    wide = block.astype(f32)
    return wide[CH : CH + 1] + wide[CH + 1 : CH + 2], wide[:CH]


def total_body(parts, total):
    state = jnp.zeros((CH, CH), f32)
    decay = jnp.zeros((1, CH), f32)
    for k in range(NQ):
        step, add = unpacked(parts[k])
        state = state * jnp.exp(step) + add
        decay = decay + step
    for k in range(total.shape[0]):
        pack(total.at[k], state, decay)


def finish_body(place, slabs, chips, inner, decayed, gain, rest, out):
    state = jnp.zeros((CH, CH), f32)
    for parts, mine in ((slabs, NQ * place[0] + place[1]), (chips, place[2])):
        for k in range(parts.shape[0]):
            step, add = unpacked(parts[k])
            state = jnp.where(k < mine, state * jnp.exp(step) + add, state)
    recurrent = inner[...] + matmul(decayed[...], state.astype(bf16), ((1,), (1,)))
    scale = lax.rsqrt(jnp.mean(recurrent * recurrent, axis=1, keepdims=True) + norm_eps)
    gate = silu(rest[:, 2 * CH :].astype(f32))
    out[...] = (recurrent * scale * own_half(gain[...], place[3]) * gate).astype(bf16)


def conv_body(place, rest, halo, taps, out, sums, gated):
    rim = halo[...].astype(f32)
    gated[:HALO] = rim[:, :CH] * sigmoid(rim[:, CH:])
    gated[HALO:] = rest[:, :CH].astype(f32) * sigmoid(rest[:, CH : 2 * CH].astype(f32))
    own_taps = own_half(taps[...], place[3])
    for n in range(ROWS // BLOCK):
        total = jnp.zeros((BLOCK, CH), f32)
        for j in range(TAPS):
            at = n * BLOCK + HALO - TAPS + 1 + j
            total = total + gated[at : at + BLOCK] * own_taps[j : j + 1]
        out[n * BLOCK : (n + 1) * BLOCK] = total.astype(bf16)
    values = out[...].astype(f32)
    ones = jnp.ones((8, CH), f32)
    first_sum = matmul(ones, values, ((1,), (1,)), HIGH)
    second_sum = matmul(ones, values * values, ((1,), (1,)), HIGH)
    row = lax.broadcasted_iota(jnp.int32, (8, ROWS), 0)
    sums[...] = jnp.where(row == 0, first_sum, second_sum)


def channel_body(place, values, s0, s1, s2, s3, gain, bias, out):
    total = s0[...] + s1[...] + s2[...] + s3[...]
    row = lax.broadcasted_iota(jnp.int32, (8, CH), 0)
    pick_first = jnp.where(row == 0, 1.0 / CONV_CH, 0.0)
    pick_second = jnp.where(row == 1, 1.0 / CONV_CH, 0.0)
    mean = matmul(total, pick_first, ((0,), (0,)), HIGH)
    variance = matmul(total, pick_second, ((0,), (0,)), HIGH) - mean * mean
    shifted = (values[...].astype(f32) - mean) * lax.rsqrt(variance + layer_eps)
    out[...] = silu(
        shifted * own_half(gain[...], place[3]) + own_half(bias[...], place[3])
    ).astype(bf16)


def output_body(place, conv_out, rec_out, columns, pieces, mine, theirs, weight, both):
    blocks = NX * NC
    step = blocks * CHUNK
    for z in range(NZ):
        piece = pieces[z, : blocks * 24].reshape(blocks, 24, CH)
        at = z * step
        weight[at : at + step, :CH] = piece[:, :CHUNK].reshape(step, CH)
        carried = columns[z, blocks * COLUMN_ROWS :].astype(f32)
        last = jnp.concatenate([carried, pieces[z, blocks * 24 :].astype(f32)], axis=0)
        second = jnp.concatenate(
            [piece[:, CHUNK:].astype(f32), last.reshape(blocks, 8, CH)], axis=1
        )
        weight[at : at + step, CH:] = second.reshape(step, CH).astype(bf16)
    both[:, :CH] = conv_out[...]
    both[:, CH:] = rec_out[...]
    for core, out in ((place[3], mine), (1 - place[3], theirs)):
        rows = pl.ds(pl.multiple_of(core * HALF, HALF), HALF)
        out[...] = matmul(both[rows], weight[...], ((1,), (1,))).astype(bf16)


def exchanged(x, axes):
    return lax.all_to_all(x, axes, split_axis=0, concat_axis=0, tiled=True)


def to_everyone(x, axes):
    copies = jnp.broadcast_to(x, (lax.axis_size(axes), *x.shape))
    return exchanged(copies, axes)


def per_device(
    tokens,
    input_norm_gain,
    convolution_value_weight,
    convolution_gate_weight,
    depthwise_filter_taps,
    channel_norm_gain,
    channel_norm_bias,
    query_projection_weight,
    forget_gate_weight,
    recurrence_value_weight,
    output_gate_weight,
    forget_floor_margin,
    decay_jump_terms,
    head_norm_gain,
    convolution_output_weight,
    recurrence_output_weight,
):
    place = jnp.stack([lax.axis_index(a) for a in SP_TP]).astype(jnp.int32)
    width = tokens.shape[1]

    payload = kernel_call(pack_body, shape((NX * NC, SENT_ROWS, CH), bf16), [VMEM] * 9)(
        query_projection_weight,
        forget_gate_weight,
        recurrence_value_weight,
        convolution_value_weight,
        convolution_gate_weight,
        output_gate_weight,
        convolution_output_weight.T,
        recurrence_output_weight.T,
        decay_jump_terms,
    )
    arrived = exchanged(payload, (X, C))
    copies = kernel_call(
        norm_body, shape((NX * NY, OWN, width), bf16), [VMEM, VMEM]
    )(tokens, input_norm_gain.reshape(1, width))
    own = exchanged(copies, (X, Y)).reshape(NX * HALF, width)
    other = lax.ppermute(own, C, [(0, 1), (1, 0)])
    along, rest_rows = kernel_call(
        sort_body, (shape((248, CH), bf16), shape((200, CH), bf16)), [VMEM]
    )(arrived)
    columns = lax.all_gather(along, (ZH, ZL), axis=0)
    out_pieces = to_everyone(rest_rows, (ZH, ZL))
    piece = shape((ROWS, 2 * CH), bf16)
    projected = kernel_call(
        project_body,
        (piece, piece, piece, piece),
        [SMEM] + [VMEM] * 3,
        [pltpu.VMEM((width, 2 * CH), bf16)],
    )(place, own, other, columns)
    pieces = [projected[0]]
    for k in range(1, NX):
        pieces.append(
            lax.ppermute(projected[k], X, [(x, (x + k) % NX) for x in range(NX)])
        )

    margin = forget_floor_margin.reshape(1, 2 * CH)
    inner, decayed, packed, rest, tail = kernel_call(
        local_body,
        (
            shape((ROWS, CH), f32),
            shape((ROWS, CH), bf16),
            shape((STATE_ROWS, CH), bf16),
            shape((ROWS, 3 * CH), bf16),
            shape((HALO, 2 * CH), bf16),
        ),
        [SMEM] + [VMEM] * 6,
    )(place, *pieces, margin, arrived)
    chips = lax.all_gather(packed, X, axis=0)

    def total_of(parts, copies):
        return kernel_call(
            total_body, shape((copies, STATE_ROWS, CH), bf16), [VMEM]
        )(parts)

    slab_copies = total_of(chips, NZ)
    slabs = exchanged(slab_copies, (ZH, ZL))

    blocks = NZ * NX
    halo = lax.ppermute(tail, (ZH, ZL, X), [(k, k + 1) for k in range(blocks - 1)])
    convolved, sums = kernel_call(
        conv_body,
        (shape((ROWS, CH), bf16), shape((8, ROWS), f32)),
        [SMEM, VMEM, VMEM, VMEM],
        [pltpu.VMEM((HALO + ROWS, CH), f32)],
    )(place, rest, halo, depthwise_filter_taps)
    sums = sums + lax.ppermute(sums, C, [(0, 1), (1, 0)])
    all_sums = [sums]
    for k in range(1, NY):
        all_sums.append(lax.ppermute(sums, Y, [(y, (y + k) % NY) for y in range(NY)]))
    conv_out = kernel_call(channel_body, shape((ROWS, CH), bf16), [SMEM] + [VMEM] * 7)(
        place,
        convolved,
        *all_sums,
        channel_norm_gain.reshape(1, 2 * CH),
        channel_norm_bias.reshape(1, 2 * CH),
    )
    rec_out = kernel_call(
        finish_body, shape((ROWS, CH), bf16), [SMEM] + [VMEM] * 6
    )(place, slabs, chips, inner, decayed, head_norm_gain.reshape(1, 2 * CH), rest)

    mine, theirs = kernel_call(
        output_body,
        (shape((HALF, width), bf16), shape((HALF, width), bf16)),
        [SMEM] + [VMEM] * 4,
        [pltpu.VMEM((width, 2 * CH), bf16), pltpu.VMEM((ROWS, 2 * CH), bf16)],
    )(place, conv_out, rec_out, columns, out_pieces)
    given = lax.ppermute(theirs, C, [(0, 1), (1, 0)])
    pair_sum = (mine.astype(f32) + given.astype(f32)).astype(bf16)
    pieces = exchanged(pair_sum.reshape(NY, OWN, width), Y)
    return pieces.astype(f32).sum(axis=0).astype(bf16)


def solution(mesh):
    split = Mesh(mesh.devices.reshape(NQ, NZ // NQ, NX, NC, mesh.shape["tp"]), SP_TP)
    return jax.shard_map(
        per_device,
        mesh=split,
        in_specs=(
            P(SP_TP, None),
            P(),
            P(SP, "tp"),
            P(SP, "tp"),
            P(None, "tp"),
            P("tp"),
            P("tp"),
            P(SP, "tp"),
            P(SP, "tp"),
            P(SP, "tp"),
            P(SP, "tp"),
            P("tp"),
            P("tp", SP),
            P("tp"),
            P("tp", SP),
            P("tp", SP),
        ),
        out_specs=P(SP_TP, None),
        check_vma=False,
    )
```

```python
import jax
import jax.numpy as jnp
from jax import lax
from jax.experimental import pallas as pl
from jax.experimental.pallas import tpu as pltpu
from jax.sharding import Mesh
from jax.sharding import PartitionSpec as P


ZH, ZL, X, C, Y = "sp_0", "sp_1", "sp_2", "sp_3", "tp"
SP = (ZH, ZL, X, C)
SP_TP = (ZH, ZL, X, C, Y)
NZ, NQ, NX, NC, NY = 16, 4, 4, 2, 4
CONV_CH = 1024
CH = 128
ROWS = 256
OWN = 32
BLOCK = 64
TAPS = 31
HALO = 32
STATE_ROWS = 40
HALF = 128
CHUNK = 16
COLUMN_ROWS = 24
OUT_ROWS = 32
SENT_ROWS = 64
norm_eps = 1e-06
layer_eps = 1e-05
HIGH = lax.Precision.HIGHEST
bf16 = jnp.bfloat16
f32 = jnp.float32

VMEM = pl.BlockSpec(memory_space=pltpu.VMEM)
SMEM = pl.BlockSpec(memory_space=pltpu.SMEM)


def kernel_call(body, out, specs, scratch=()):
    return pl.pallas_call(
        body,
        out_shape=out,
        in_specs=specs,
        out_specs=jax.tree.map(lambda _: VMEM, out),
        scratch_shapes=scratch,
    )


def shape(dims, dtype):
    return jax.ShapeDtypeStruct(dims, dtype)


def matmul(a, b, dims, precision=None):
    return lax.dot_general(
        a, b, (dims, ((), ())), precision=precision, preferred_element_type=f32
    )


def sigmoid(v):
    return 1.0 / (1.0 + jnp.exp(-v))


def silu(v):
    return v * sigmoid(v)


def own_half(value, core):
    return jnp.where(core == 0, value[:, :CH], value[:, CH:])


def pack_body(query, forget, value, left, gate, outgate, conv_out, rec_out, jump, out):
    whole = (query, value, left, outgate)
    split = (forget, forget, gate, gate)
    lane = lax.broadcasted_iota(jnp.int32, (8, CH), 1)
    for c in range(NC):
        half = slice(c * CH, (c + 1) * CH)
        row = jnp.broadcast_to(jump[c : c + 1], (8, CH))
        high = row.astype(bf16).astype(f32)
        first = lax.broadcasted_iota(jnp.int32, (8, CH), 0)
        jumps = jnp.where(first == 0, high, row - high).astype(bf16)
        for x in range(NX):
            to = NC * x + c
            out[to, :CHUNK] = whole[x][:, half]
            rows = split[x][:, half].astype(f32)
            turned = pltpu.roll(rows[8:], CH // 2, 1)
            keep = lane < CH // 2 if x % 2 == 0 else lane >= CH // 2
            out[to, CHUNK:COLUMN_ROWS] = jnp.where(keep, rows[:8], turned).astype(bf16)
            out[to, COLUMN_ROWS : COLUMN_ROWS + CHUNK] = conv_out[:, half]
            out[to, COLUMN_ROWS + CHUNK : COLUMN_ROWS + OUT_ROWS] = rec_out[:, half]
            out[to, COLUMN_ROWS + OUT_ROWS :] = jumps


def norm_body(tokens, gain, out):
    features = tokens[...].astype(f32)
    normed = (
        features
        * lax.rsqrt(jnp.mean(features * features, axis=1, keepdims=True) + norm_eps)
        * gain[...]
    ).astype(bf16)
    for k in range(NX * NY):
        out[k] = normed


def project_body(place, own, other, columns, out, weight):
    c = place[3]
    blocks = NX * NC
    step = blocks * CHUNK
    for z in range(NZ):
        at = z * step
        piece = columns[z * blocks : (z + 1) * blocks]
        weight[at : at + step, :CH] = piece[:, :CHUNK].reshape(step, CH)
        packed = piece[:, CHUNK:].reshape(blocks * 8, CH).astype(f32)
        turned = pltpu.roll(packed, CH // 2, 1).reshape(blocks, 8, CH)
        both = jnp.concatenate([packed.reshape(blocks, 8, CH), turned], axis=1)
        weight[at : at + step, CH:] = both.reshape(step, CH).astype(bf16)
    for x in range(NX):
        rows = slice(x * HALF, (x + 1) * HALF)
        for core, tokens in ((c, own), (1 - c, other)):
            to = pl.ds(pl.multiple_of(core * HALF, HALF), HALF)
            out[x, to] = matmul(tokens[rows], weight[...], ((1,), (0,))).astype(bf16)


def joined(pieces, x):
    lane = lax.broadcasted_iota(jnp.int32, (ROWS, CH), 1)
    first, second = (pieces[k, :, CH:].astype(f32) for k in (x, x + 1))
    return jnp.where(lane < CH // 2, first, second)


def local_body(place, pieces, margin, arrived, inner, decayed, packed, rest, tail):
    c = place[3]
    at = COLUMN_ROWS + OUT_ROWS
    rows = [arrived[NC * place[2] + k, at : at + 8].astype(f32) for k in range(NC)]
    jump = jnp.concatenate([r[:1] + r[1:2] for r in rows], axis=1)
    bound = own_half(margin[...], c)
    queries = silu(pieces[0, :, :CH].astype(f32))
    keys = bound * sigmoid(-joined(pieces, 0))
    inputs = pieces[1, :, :CH]
    others = (
        pieces[2, :, :CH].astype(f32),
        joined(pieces, 2),
        pieces[3, :, :CH].astype(f32),
    )
    for k, value in enumerate(others):
        rest[:, k * CH : (k + 1) * CH] = value.astype(bf16)
        if k < 2:
            tail[:, k * CH : (k + 1) * CH] = value[ROWS - HALO :].astype(bf16)
    log_forget = jnp.log1p(-keys)
    row = lax.broadcasted_iota(jnp.int32, (BLOCK, BLOCK), 0)
    col = lax.broadcasted_iota(jnp.int32, (BLOCK, BLOCK), 1)
    causal = row >= col
    lower = jnp.where(causal, 1.0, 0.0)
    state = jnp.zeros((CH, CH), f32)
    before = jnp.zeros((1, CH), f32)
    for n in range(ROWS // BLOCK):
        at = slice(n * BLOCK, (n + 1) * BLOCK)
        jumps = jump[:, n * BLOCK : (n + 1) * BLOCK]
        jumped = jnp.sum(jnp.where(causal, jumps, 0.0), axis=1, keepdims=True)
        running = matmul(lower, log_forget[at], ((1,), (0,)), HIGH) + jumped
        final = running[BLOCK - 1 : BLOCK]
        scaled = queries[at] * jnp.exp(running)
        scaled_keys = (keys[at] * jnp.exp(-running)).astype(bf16)
        final_keys = (keys[at] * jnp.exp(final - running)).astype(bf16)
        scores = matmul(scaled.astype(bf16), scaled_keys, ((1,), (1,)))
        scores = jnp.where(causal, scores, 0.0).astype(bf16)
        inner[at] = matmul(scores, inputs[at], ((1,), (0,))) + matmul(
            scaled.astype(bf16), state.astype(bf16), ((1,), (1,))
        )
        decayed[at] = (scaled * jnp.exp(before)).astype(bf16)
        state = state * jnp.exp(final) + matmul(inputs[at], final_keys, ((0,), (0,)))
        before = before + final
    high = before.astype(bf16)
    low = (before - high.astype(f32)).astype(bf16)
    first = lax.broadcasted_iota(jnp.int32, (8, CH), 0)
    tail = jnp.where(first == 0, high.astype(f32), jnp.where(first == 1, low.astype(f32), 0.0))
    for x in range(NX):
        packed[x, :OWN] = state[x * OWN : (x + 1) * OWN].astype(bf16)
        packed[x, OWN:] = tail.astype(bf16)


def unpacked(block):
    wide = block.astype(f32)
    return wide[OWN : OWN + 1] + wide[OWN + 1 : OWN + 2], wide[:OWN]


def slab_body(parts, total):
    state = jnp.zeros((OWN, CH), f32)
    decay = jnp.zeros((1, CH), f32)
    for x in range(NX):
        step, add = unpacked(parts[x])
        state = state * jnp.exp(step) + add
        decay = decay + step
    high = decay.astype(bf16).astype(f32)
    low = decay - high
    first = lax.broadcasted_iota(jnp.int32, (8, CH), 0)
    tail = jnp.where(first == 0, high, jnp.where(first == 1, low, 0.0)).astype(bf16)
    for z in range(NZ):
        total[z, :OWN] = state.astype(bf16)
        total[z, OWN:] = tail


def prefix_body(place, slabs, parts, starts):
    mine = NQ * place[0] + place[1]
    state = jnp.zeros((OWN, CH), f32)
    for z in range(NZ):
        step, add = unpacked(slabs[z])
        state = jnp.where(z < mine, state * jnp.exp(step) + add, state)
    for x in range(NX):
        starts[x] = state.astype(bf16)
        step, add = unpacked(parts[x])
        state = state * jnp.exp(step) + add


def finish_body(place, inner, decayed, start, gain, rest, out):
    recurrent = inner[...] + matmul(decayed[...], start[...], ((1,), (1,)))
    scale = lax.rsqrt(jnp.mean(recurrent * recurrent, axis=1, keepdims=True) + norm_eps)
    gate = silu(rest[:, 2 * CH :].astype(f32))
    out[...] = (recurrent * scale * own_half(gain[...], place[3]) * gate).astype(bf16)


def conv_body(place, rest, halo, taps, out, sums, gated):
    rim = halo[...].astype(f32)
    gated[:HALO] = rim[:, :CH] * sigmoid(rim[:, CH:])
    gated[HALO:] = rest[:, :CH].astype(f32) * sigmoid(rest[:, CH : 2 * CH].astype(f32))
    own_taps = own_half(taps[...], place[3])
    for n in range(ROWS // BLOCK):
        total = jnp.zeros((BLOCK, CH), f32)
        for j in range(TAPS):
            at = n * BLOCK + HALO - TAPS + 1 + j
            total = total + gated[at : at + BLOCK] * own_taps[j : j + 1]
        out[n * BLOCK : (n + 1) * BLOCK] = total.astype(bf16)
    values = out[...].astype(f32)
    ones = jnp.ones((8, CH), f32)
    first_sum = matmul(ones, values, ((1,), (1,)), HIGH)
    second_sum = matmul(ones, values * values, ((1,), (1,)), HIGH)
    row = lax.broadcasted_iota(jnp.int32, (8, ROWS), 0)
    both_sums = jnp.where(row == 0, first_sum, second_sum)
    for k in range(NC * NY):
        sums[k] = both_sums


def channel_body(place, values, sums, gain, bias, out):
    total = sums[0]
    for k in range(1, NC * NY):
        total = total + sums[k]
    row = lax.broadcasted_iota(jnp.int32, (8, CH), 0)
    pick_first = jnp.where(row == 0, 1.0 / CONV_CH, 0.0)
    pick_second = jnp.where(row == 1, 1.0 / CONV_CH, 0.0)
    mean = matmul(total, pick_first, ((0,), (0,)), HIGH)
    variance = matmul(total, pick_second, ((0,), (0,)), HIGH) - mean * mean
    shifted = (values[...].astype(f32) - mean) * lax.rsqrt(variance + layer_eps)
    out[...] = silu(
        shifted * own_half(gain[...], place[3]) + own_half(bias[...], place[3])
    ).astype(bf16)


def output_body(place, conv_out, rec_out, pieces, mine, theirs, weight, both):
    blocks = NX * NC
    step = blocks * CHUNK
    for z in range(NZ):
        at = z * step
        piece = pieces[z]
        weight[at : at + step, :CH] = piece[:, :CHUNK].reshape(step, CH)
        weight[at : at + step, CH:] = piece[:, CHUNK:].reshape(step, CH)
    both[:, :CH] = conv_out[...]
    both[:, CH:] = rec_out[...]
    for core, out in ((place[3], mine), (1 - place[3], theirs)):
        rows = pl.ds(pl.multiple_of(core * HALF, HALF), HALF)
        out[...] = matmul(both[rows], weight[...], ((1,), (1,))).astype(bf16)


def exchanged(x, axes):
    return lax.all_to_all(x, axes, split_axis=0, concat_axis=0, tiled=True)


def per_device(
    tokens,
    input_norm_gain,
    convolution_value_weight,
    convolution_gate_weight,
    depthwise_filter_taps,
    channel_norm_gain,
    channel_norm_bias,
    query_projection_weight,
    forget_gate_weight,
    recurrence_value_weight,
    output_gate_weight,
    forget_floor_margin,
    decay_jump_terms,
    head_norm_gain,
    convolution_output_weight,
    recurrence_output_weight,
):
    place = jnp.stack([lax.axis_index(a) for a in SP_TP]).astype(jnp.int32)
    width = tokens.shape[1]

    payload = kernel_call(pack_body, shape((NX * NC, SENT_ROWS, CH), bf16), [VMEM] * 9)(
        query_projection_weight,
        forget_gate_weight,
        recurrence_value_weight,
        convolution_value_weight,
        convolution_gate_weight,
        output_gate_weight,
        convolution_output_weight.T,
        recurrence_output_weight.T,
        decay_jump_terms,
    )
    arrived = exchanged(payload, (X, C))
    copies = kernel_call(
        norm_body, shape((NX * NY, OWN, width), bf16), [VMEM, VMEM]
    )(tokens, input_norm_gain.reshape(1, width))
    own = exchanged(copies, (X, Y)).reshape(NX * HALF, width)
    other = lax.ppermute(own, C, [(0, 1), (1, 0)])
    columns = lax.all_gather(arrived[:, :COLUMN_ROWS], (ZH, ZL), axis=0, tiled=True)
    out_pieces = lax.all_gather(
        arrived[:, COLUMN_ROWS : COLUMN_ROWS + OUT_ROWS], (ZH, ZL), axis=0
    )
    projected = kernel_call(
        project_body,
        shape((NX, ROWS, 2 * CH), bf16),
        [SMEM] + [VMEM] * 3,
        [pltpu.VMEM((width, 2 * CH), bf16)],
    )(place, own, other, columns)
    pieces = exchanged(projected, X)

    margin = forget_floor_margin.reshape(1, 2 * CH)
    inner, decayed, packed, rest, tail = kernel_call(
        local_body,
        (
            shape((ROWS, CH), f32),
            shape((ROWS, CH), bf16),
            shape((NX, STATE_ROWS, CH), bf16),
            shape((ROWS, 3 * CH), bf16),
            shape((HALO, 2 * CH), bf16),
        ),
        [SMEM] + [VMEM] * 3,
    )(place, pieces, margin, arrived)
    parts = exchanged(packed, X)
    slab_copies = kernel_call(
        slab_body, shape((NZ, STATE_ROWS, CH), bf16), [VMEM]
    )(parts)
    slabs = exchanged(slab_copies, (ZH, ZL))
    starts = kernel_call(
        prefix_body, shape((NX, OWN, CH), bf16), [SMEM, VMEM, VMEM]
    )(place, slabs, parts)
    start = exchanged(starts, X).reshape(CH, CH)

    blocks = NZ * NX
    halo = lax.ppermute(tail, (ZH, ZL, X), [(k, k + 1) for k in range(blocks - 1)])
    convolved, sums = kernel_call(
        conv_body,
        (shape((ROWS, CH), bf16), shape((NC * NY, 8, ROWS), f32)),
        [SMEM, VMEM, VMEM, VMEM],
        [pltpu.VMEM((HALO + ROWS, CH), f32)],
    )(place, rest, halo, depthwise_filter_taps)
    all_sums = exchanged(sums, (C, Y))
    conv_out = kernel_call(channel_body, shape((ROWS, CH), bf16), [SMEM] + [VMEM] * 4)(
        place,
        convolved,
        all_sums,
        channel_norm_gain.reshape(1, 2 * CH),
        channel_norm_bias.reshape(1, 2 * CH),
    )
    rec_out = kernel_call(
        finish_body, shape((ROWS, CH), bf16), [SMEM] + [VMEM] * 5
    )(place, inner, decayed, start, head_norm_gain.reshape(1, 2 * CH), rest)

    mine, theirs = kernel_call(
        output_body,
        (shape((HALF, width), bf16), shape((HALF, width), bf16)),
        [SMEM] + [VMEM] * 3,
        [pltpu.VMEM((width, 2 * CH), bf16), pltpu.VMEM((ROWS, 2 * CH), bf16)],
    )(place, conv_out, rec_out, out_pieces)
    given = lax.ppermute(theirs, C, [(0, 1), (1, 0)])
    pair_sum = (mine.astype(f32) + given.astype(f32)).astype(bf16)
    pieces = exchanged(pair_sum.reshape(NY, OWN, width), Y)
    return pieces.astype(f32).sum(axis=0).astype(bf16)


def solution(mesh):
    split = Mesh(mesh.devices.reshape(NQ, NZ // NQ, NX, NC, mesh.shape["tp"]), SP_TP)
    return jax.shard_map(
        per_device,
        mesh=split,
        in_specs=(
            P(SP_TP, None),
            P(),
            P(SP, "tp"),
            P(SP, "tp"),
            P(None, "tp"),
            P("tp"),
            P("tp"),
            P(SP, "tp"),
            P(SP, "tp"),
            P(SP, "tp"),
            P(SP, "tp"),
            P("tp"),
            P("tp", SP),
            P("tp"),
            P("tp", SP),
            P("tp", SP),
        ),
        out_specs=P(SP_TP, None),
        check_vma=False,
    )
```

```python
import jax
import jax.numpy as jnp
from jax import lax
from jax.experimental import pallas as pl
from jax.experimental.pallas import tpu as pltpu
from jax.sharding import Mesh
from jax.sharding import PartitionSpec as P


ZH, ZL, X, C, Y = "sp_0", "sp_1", "sp_2", "sp_3", "tp"
SP = (ZH, ZL, X, C)
SP_TP = (ZH, ZL, X, C, Y)
NZ, NQ, NX, NC, NY = 16, 4, 4, 2, 4
CONV_CH = 1024
CH = 128
ROWS = 256
OWN = 32
BLOCK = 64
TAPS = 31
HALO = 32
STATE_ROWS = 40
HALF = 128
CHUNK = 16
COLUMN_ROWS = 24
OUT_ROWS = 32
SENT_ROWS = 64
norm_eps = 1e-06
layer_eps = 1e-05
HIGH = lax.Precision.HIGHEST
bf16 = jnp.bfloat16
f32 = jnp.float32

VMEM = pl.BlockSpec(memory_space=pltpu.VMEM)
SMEM = pl.BlockSpec(memory_space=pltpu.SMEM)


def kernel_call(body, out, specs, scratch=()):
    return pl.pallas_call(
        body,
        out_shape=out,
        in_specs=specs,
        out_specs=jax.tree.map(lambda _: VMEM, out),
        scratch_shapes=scratch,
    )


def shape(dims, dtype):
    return jax.ShapeDtypeStruct(dims, dtype)


def matmul(a, b, dims, precision=None):
    return lax.dot_general(
        a, b, (dims, ((), ())), precision=precision, preferred_element_type=f32
    )


def sigmoid(v):
    return 1.0 / (1.0 + jnp.exp(-v))


def silu(v):
    return v * sigmoid(v)


def own_half(value, core):
    return jnp.where(core == 0, value[:, :CH], value[:, CH:])


def pack_body(query, forget, value, left, gate, outgate, conv_out, rec_out, jump, out):
    whole = (query, value, left, outgate)
    split = (forget, forget, gate, gate)
    lane = lax.broadcasted_iota(jnp.int32, (8, CH), 1)
    for c in range(NC):
        half = slice(c * CH, (c + 1) * CH)
        row = jnp.broadcast_to(jump[c : c + 1], (8, CH))
        high = row.astype(bf16).astype(f32)
        first = lax.broadcasted_iota(jnp.int32, (8, CH), 0)
        jumps = jnp.where(first == 0, high, row - high).astype(bf16)
        for x in range(NX):
            to = NC * x + c
            out[to, :CHUNK] = whole[x][:, half]
            rows = split[x][:, half].astype(f32)
            turned = pltpu.roll(rows[8:], CH // 2, 1)
            keep = lane < CH // 2 if x % 2 == 0 else lane >= CH // 2
            out[to, CHUNK:COLUMN_ROWS] = jnp.where(keep, rows[:8], turned).astype(bf16)
            out[to, COLUMN_ROWS : COLUMN_ROWS + CHUNK] = conv_out[:, half]
            out[to, COLUMN_ROWS + CHUNK : COLUMN_ROWS + OUT_ROWS] = rec_out[:, half]
            out[to, COLUMN_ROWS + OUT_ROWS :] = jumps


def norm_body(tokens, gain, out):
    features = tokens[...].astype(f32)
    normed = (
        features
        * lax.rsqrt(jnp.mean(features * features, axis=1, keepdims=True) + norm_eps)
        * gain[...]
    ).astype(bf16)
    for k in range(NX * NY):
        out[k] = normed


def weight_body(own, columns, half, weight):
    blocks = NX * NC
    step = blocks * CHUNK
    for z in range(NZ):
        at = z * step
        piece = columns[z * blocks : (z + 1) * blocks]
        weight[at : at + step, :CH] = piece[:, :CHUNK].reshape(step, CH)
        packed = piece[:, CHUNK:].reshape(blocks * 8, CH).astype(f32)
        turned = pltpu.roll(packed, CH // 2, 1).reshape(blocks, 8, CH)
        both = jnp.concatenate([packed.reshape(blocks, 8, CH), turned], axis=1)
        weight[at : at + step, CH:] = both.reshape(step, CH).astype(bf16)
    half[...] = matmul(own[...], weight[...], ((1,), (0,))).astype(bf16)


def project_body(place, other, half, weight, out):
    c = place[3]
    even = lax.rem(place[2], 2) == 0
    result = matmul(other[...], weight[...], ((1,), (0,))).astype(bf16)
    lane = lax.broadcasted_iota(jnp.int32, (HALF, CH), 1)
    keep = (lane < CH // 2) == even
    for x in range(NX):
        rows = slice(x * HALF, (x + 1) * HALF)
        mine, theirs = half[rows], result[rows]
        out[x, pl.ds(pl.multiple_of(c * HALF, HALF), HALF)] = mine[:, :CH]
        out[x, pl.ds(pl.multiple_of((1 - c) * HALF, HALF), HALF)] = theirs[:, :CH]
        mine, theirs = mine[:, CH:].astype(f32), theirs[:, CH:].astype(f32)
        early = jnp.where(c == 0, mine, theirs)
        late = jnp.where(c == 0, theirs, mine)
        out[x, ROWS:] = jnp.where(keep, early, pltpu.roll(late, CH // 2, 1)).astype(bf16)


def joined(pieces, x):
    lane = lax.broadcasted_iota(jnp.int32, (HALF, CH), 1)
    first, second = (pieces[k, ROWS:].astype(f32) for k in (x, x + 1))
    early = jnp.where(lane < CH // 2, first, second)
    late = pltpu.roll(jnp.where(lane < CH // 2, second, first), CH // 2, 1)
    return jnp.concatenate([early, late], axis=0)


def gates_of(pieces, margin, arrived, place):
    at = COLUMN_ROWS + OUT_ROWS
    rows = [arrived[NC * place[2] + k, at : at + 8].astype(f32) for k in range(NC)]
    jump = jnp.concatenate([r[:1] + r[1:2] for r in rows], axis=1)
    keys = own_half(margin[...], place[3]) * sigmoid(-joined(pieces, 0))
    log_forget = jnp.log1p(-keys)
    row = lax.broadcasted_iota(jnp.int32, (BLOCK, BLOCK), 0)
    col = lax.broadcasted_iota(jnp.int32, (BLOCK, BLOCK), 1)
    causal = row >= col
    lower = jnp.where(causal, 1.0, 0.0)
    running = []
    for n in range(ROWS // BLOCK):
        jumps = jump[:, n * BLOCK : (n + 1) * BLOCK]
        jumped = jnp.sum(jnp.where(causal, jumps, 0.0), axis=1, keepdims=True)
        part = log_forget[n * BLOCK : (n + 1) * BLOCK]
        running.append(matmul(lower, part, ((1,), (0,)), HIGH) + jumped)
    return keys, running, causal


def state_body(place, pieces, margin, arrived, packed, tail):
    keys, running, _ = gates_of(pieces, margin, arrived, place)
    inputs = pieces[1, :ROWS]
    state = jnp.zeros((CH, CH), f32)
    decay = jnp.zeros((1, CH), f32)
    for n in range(ROWS // BLOCK):
        at = slice(n * BLOCK, (n + 1) * BLOCK)
        final = running[n][BLOCK - 1 : BLOCK]
        final_keys = (keys[at] * jnp.exp(final - running[n])).astype(bf16)
        state = state * jnp.exp(final) + matmul(inputs[at], final_keys, ((0,), (0,)))
        decay = decay + final
    high = decay.astype(bf16).astype(f32)
    low = decay - high
    first = lax.broadcasted_iota(jnp.int32, (8, CH), 0)
    sent = jnp.where(first == 0, high, jnp.where(first == 1, low, 0.0)).astype(bf16)
    for x in range(NX):
        packed[x, :OWN] = state[x * OWN : (x + 1) * OWN].astype(bf16)
        packed[x, OWN:] = sent
    tail[:, :CH] = pieces[2, ROWS - HALO : ROWS]
    tail[:, CH:] = joined(pieces, 2)[ROWS - HALO :].astype(bf16)


def local_body(place, pieces, margin, arrived, inner, decayed):
    keys, running, causal = gates_of(pieces, margin, arrived, place)
    queries = silu(pieces[0, :ROWS].astype(f32))
    inputs = pieces[1, :ROWS]
    state = jnp.zeros((CH, CH), f32)
    before = jnp.zeros((1, CH), f32)
    for n in range(ROWS // BLOCK):
        at = slice(n * BLOCK, (n + 1) * BLOCK)
        final = running[n][BLOCK - 1 : BLOCK]
        scaled = queries[at] * jnp.exp(running[n])
        scaled_keys = (keys[at] * jnp.exp(-running[n])).astype(bf16)
        final_keys = (keys[at] * jnp.exp(final - running[n])).astype(bf16)
        scores = matmul(scaled.astype(bf16), scaled_keys, ((1,), (1,)))
        scores = jnp.where(causal, scores, 0.0).astype(bf16)
        inner[at] = matmul(scores, inputs[at], ((1,), (0,))) + matmul(
            scaled.astype(bf16), state.astype(bf16), ((1,), (1,))
        )
        decayed[at] = (scaled * jnp.exp(before)).astype(bf16)
        state = state * jnp.exp(final) + matmul(inputs[at], final_keys, ((0,), (0,)))
        before = before + final


def unpacked(block):
    wide = block.astype(f32)
    return wide[OWN : OWN + 1] + wide[OWN + 1 : OWN + 2], wide[:OWN]


def slab_body(parts, total):
    state = jnp.zeros((OWN, CH), f32)
    decay = jnp.zeros((1, CH), f32)
    for x in range(NX):
        step, add = unpacked(parts[x])
        state = state * jnp.exp(step) + add
        decay = decay + step
    high = decay.astype(bf16).astype(f32)
    low = decay - high
    first = lax.broadcasted_iota(jnp.int32, (8, CH), 0)
    tail = jnp.where(first == 0, high, jnp.where(first == 1, low, 0.0)).astype(bf16)
    for z in range(NZ):
        total[z, :OWN] = state.astype(bf16)
        total[z, OWN:] = tail


def bridge_body(place, slabs, parts, sums, out):
    mine = NQ * place[0] + place[1]
    own = NY * place[3] + place[4]
    state = jnp.zeros((OWN, CH), f32)
    for z in range(NZ):
        step, add = unpacked(slabs[z])
        state = jnp.where(z < mine, state * jnp.exp(step) + add, state)
    row = lax.broadcasted_iota(jnp.int32, (8, CH), 0)
    packed = []
    for k in range(2):
        value = sums[:, k * CH : (k + 1) * CH]
        high = value.astype(bf16).astype(f32)
        middle = (value - high).astype(bf16).astype(f32)
        low = value - high - middle
        packed.append(jnp.where(row < 2, high, jnp.where(row < 4, middle, low)))
    packed = jnp.concatenate([*packed, jnp.zeros((16, CH), f32)], axis=0)
    for x in range(NX):
        for k in range(NC * NY):
            out[x * NC * NY + k] = jnp.where(k == own, state, packed).astype(bf16)
        step, add = unpacked(parts[x])
        state = state * jnp.exp(step) + add


def conv_body(place, pieces, halo, taps, out, sums, gated):
    rim = halo[...].astype(f32)
    gated[:HALO] = rim[:, :CH] * sigmoid(rim[:, CH:])
    gated[HALO:] = pieces[2, :ROWS].astype(f32) * sigmoid(joined(pieces, 2))
    own_taps = own_half(taps[...], place[3])
    for n in range(ROWS // BLOCK):
        total = jnp.zeros((BLOCK, CH), f32)
        for j in range(TAPS):
            at = n * BLOCK + HALO - TAPS + 1 + j
            total = total + gated[at : at + BLOCK] * own_taps[j : j + 1]
        out[n * BLOCK : (n + 1) * BLOCK] = total.astype(bf16)
    values = out[...].astype(f32)
    ones = jnp.ones((8, CH), f32)
    first_sum = matmul(ones, values, ((1,), (1,)), HIGH)
    second_sum = matmul(ones, values * values, ((1,), (1,)), HIGH)
    row = lax.broadcasted_iota(jnp.int32, (8, ROWS), 0)
    sums[...] = jnp.where(row % 2 == 0, first_sum, second_sum)


def order_body(pieces, weight):
    blocks = NX * NC
    step = blocks * CHUNK
    for z in range(NZ):
        at = z * step
        piece = pieces[z]
        weight[at : at + step, :CH] = piece[:, :CHUNK].reshape(step, CH)
        weight[at : at + step, CH:] = piece[:, CHUNK:].reshape(step, CH)


def tail_body(
    place, joint, sums, values, gain, bias, inner, decayed, head_gain, pieces, weight, mine, theirs, both
):
    c = place[3]
    group = NC * NY
    own = NY * c + place[4]
    total = jnp.zeros((8, ROWS), f32)
    for k in range(group):
        piece = joint[group * place[2] + k].astype(f32)
        part = jnp.concatenate([piece[:8], piece[8:16]], axis=1)
        total = total + jnp.where(k == own, 0.0, part)
    row = lax.broadcasted_iota(jnp.int32, (8, ROWS), 0)
    total = total + jnp.where(row < 2, sums[...], 0.0)
    row = lax.broadcasted_iota(jnp.int32, (8, CH), 0)
    pick_first = jnp.where((row < 6) & (row % 2 == 0), 1.0 / CONV_CH, 0.0)
    pick_second = jnp.where((row < 6) & (row % 2 == 1), 1.0 / CONV_CH, 0.0)
    mean = matmul(total, pick_first, ((0,), (0,)), HIGH)
    variance = matmul(total, pick_second, ((0,), (0,)), HIGH) - mean * mean
    shifted = (values[...].astype(f32) - mean) * lax.rsqrt(variance + layer_eps)
    both[:, :CH] = silu(shifted * own_half(gain[...], c) + own_half(bias[...], c)).astype(bf16)
    start = jnp.concatenate([joint[group * x + own] for x in range(NX)], axis=0)
    recurrent = inner[...] + matmul(decayed[...], start, ((1,), (1,)))
    scale = lax.rsqrt(jnp.mean(recurrent * recurrent, axis=1, keepdims=True) + norm_eps)
    gate = silu(pieces[3, :ROWS].astype(f32))
    both[:, CH:] = (recurrent * scale * own_half(head_gain[...], c) * gate).astype(bf16)
    for core, out in ((c, mine), (1 - c, theirs)):
        rows = pl.ds(pl.multiple_of(core * HALF, HALF), HALF)
        out[...] = matmul(both[rows], weight[...], ((1,), (1,))).astype(bf16)


def exchanged(x, axes):
    return lax.all_to_all(x, axes, split_axis=0, concat_axis=0, tiled=True)


def per_device(
    tokens,
    input_norm_gain,
    convolution_value_weight,
    convolution_gate_weight,
    depthwise_filter_taps,
    channel_norm_gain,
    channel_norm_bias,
    query_projection_weight,
    forget_gate_weight,
    recurrence_value_weight,
    output_gate_weight,
    forget_floor_margin,
    decay_jump_terms,
    head_norm_gain,
    convolution_output_weight,
    recurrence_output_weight,
):
    place = jnp.stack([lax.axis_index(a) for a in SP_TP]).astype(jnp.int32)
    width = tokens.shape[1]

    payload = kernel_call(pack_body, shape((NX * NC, SENT_ROWS, CH), bf16), [VMEM] * 9)(
        query_projection_weight,
        forget_gate_weight,
        recurrence_value_weight,
        convolution_value_weight,
        convolution_gate_weight,
        output_gate_weight,
        convolution_output_weight.T,
        recurrence_output_weight.T,
        decay_jump_terms,
    )
    arrived = exchanged(payload, (X, C))
    copies = kernel_call(
        norm_body, shape((NX * NY, OWN, width), bf16), [VMEM, VMEM]
    )(tokens, input_norm_gain.reshape(1, width))
    own = exchanged(copies, (X, Y)).reshape(NX * HALF, width)
    other = lax.ppermute(own, C, [(0, 1), (1, 0)])
    columns = lax.all_gather(arrived[:, :COLUMN_ROWS], (ZH, ZL), axis=0, tiled=True)
    out_pieces = lax.all_gather(
        arrived[:, COLUMN_ROWS : COLUMN_ROWS + OUT_ROWS], (ZH, ZL), axis=0
    )
    half, weight = kernel_call(
        weight_body,
        (shape((NX * HALF, 2 * CH), bf16), shape((width, 2 * CH), bf16)),
        [VMEM] * 2,
    )(own, columns)
    projected = kernel_call(
        project_body, shape((NX, ROWS + HALF, CH), bf16), [SMEM] + [VMEM] * 3
    )(place, other, half, weight)
    pieces = exchanged(projected, X)

    margin = forget_floor_margin.reshape(1, 2 * CH)
    packed, tail = kernel_call(
        state_body,
        (shape((NX, STATE_ROWS, CH), bf16), shape((HALO, 2 * CH), bf16)),
        [SMEM] + [VMEM] * 3,
    )(place, pieces, margin, arrived)
    inner, decayed = kernel_call(
        local_body,
        (shape((ROWS, CH), f32), shape((ROWS, CH), bf16)),
        [SMEM] + [VMEM] * 3,
    )(place, pieces, margin, arrived)
    parts = exchanged(packed, X)
    slab_copies = kernel_call(
        slab_body, shape((NZ, STATE_ROWS, CH), bf16), [VMEM]
    )(parts)
    slabs = exchanged(slab_copies, (ZH, ZL))
    blocks = NZ * NX
    halo = lax.ppermute(tail, (ZH, ZL, X), [(k, k + 1) for k in range(blocks - 1)])
    convolved, sums = kernel_call(
        conv_body,
        (shape((ROWS, CH), bf16), shape((8, ROWS), f32)),
        [SMEM, VMEM, VMEM, VMEM],
        [pltpu.VMEM((HALO + ROWS, CH), f32)],
    )(place, pieces, halo, depthwise_filter_taps)
    bridge = kernel_call(
        bridge_body, shape((NX * NC * NY, OWN, CH), bf16), [SMEM] + [VMEM] * 3
    )(place, slabs, parts, sums)
    joint = exchanged(bridge, (X, C, Y))
    out_weight = kernel_call(order_body, shape((width, 2 * CH), bf16), [VMEM])(
        out_pieces
    )
    mine, theirs = kernel_call(
        tail_body,
        (shape((HALF, width), bf16), shape((HALF, width), bf16)),
        [SMEM] + [VMEM] * 10,
        [pltpu.VMEM((ROWS, 2 * CH), bf16)],
    )(
        place,
        joint,
        sums,
        convolved,
        channel_norm_gain.reshape(1, 2 * CH),
        channel_norm_bias.reshape(1, 2 * CH),
        inner,
        decayed,
        head_norm_gain.reshape(1, 2 * CH),
        pieces,
        out_weight,
    )
    given = lax.ppermute(theirs, C, [(0, 1), (1, 0)])
    pair_sum = (mine.astype(f32) + given.astype(f32)).astype(bf16)
    pieces = exchanged(pair_sum.reshape(NY, OWN, width), Y)
    return pieces.astype(f32).sum(axis=0).astype(bf16)


def solution(mesh):
    split = Mesh(mesh.devices.reshape(NQ, NZ // NQ, NX, NC, mesh.shape["tp"]), SP_TP)
    return jax.shard_map(
        per_device,
        mesh=split,
        in_specs=(
            P(SP_TP, None),
            P(),
            P(SP, "tp"),
            P(SP, "tp"),
            P(None, "tp"),
            P("tp"),
            P("tp"),
            P(SP, "tp"),
            P(SP, "tp"),
            P(SP, "tp"),
            P(SP, "tp"),
            P("tp"),
            P("tp", SP),
            P("tp"),
            P("tp", SP),
            P("tp", SP),
        ),
        out_specs=P(SP_TP, None),
        check_vma=False,
    )
```

```python
import jax
import jax.numpy as jnp
from jax import lax
from jax.experimental import pallas as pl
from jax.experimental.pallas import tpu as pltpu
from jax.sharding import Mesh
from jax.sharding import PartitionSpec as P


ZH, ZL, X, C, Y = "sp_0", "sp_1", "sp_2", "sp_3", "tp"
SP = (ZH, ZL, X, C)
SP_TP = (ZH, ZL, X, C, Y)
NZ, NQ, NX, NC, NY = 16, 4, 4, 2, 4
CONV_CH = 1024
CH = 128
ROWS = 256
OWN = 32
BLOCK = 64
TAPS = 31
HALO = 32
STATE_ROWS = 40
LIMIT = 16 * 2**20
HALF = 128
CHUNK = 16
COLUMN_ROWS = 24
OUT_ROWS = 32
SENT_ROWS = 64
norm_eps = 1e-06
layer_eps = 1e-05
HIGH = lax.Precision.HIGHEST
bf16 = jnp.bfloat16
f32 = jnp.float32

VMEM = pl.BlockSpec(memory_space=pltpu.VMEM)
SMEM = pl.BlockSpec(memory_space=pltpu.SMEM)


def in_vmem(value, spec):
    if spec is SMEM or not isinstance(value, jax.Array):
        return value
    return pltpu.with_memory_space_constraint(value, pltpu.VMEM)


def kernel_call(body, out, specs, scratch=(), near=True):
    call = pl.pallas_call(
        body,
        out_shape=jax.tree.map(lambda o: pltpu.VMEM(o.shape, o.dtype), out) if near else out,
        in_specs=specs,
        out_specs=jax.tree.map(lambda _: VMEM, out),
        scratch_shapes=scratch,
        compiler_params=pltpu.CompilerParams(vmem_limit_bytes=LIMIT if near else None),
    )
    if not near:
        return call
    return lambda *args: call(*[in_vmem(a, s) for a, s in zip(args, specs)])


def shape(dims, dtype):
    return jax.ShapeDtypeStruct(dims, dtype)


def matmul(a, b, dims, precision=None):
    return lax.dot_general(
        a, b, (dims, ((), ())), precision=precision, preferred_element_type=f32
    )


def sigmoid(v):
    return 1.0 / (1.0 + jnp.exp(-v))


def silu(v):
    return v * sigmoid(v)


def own_half(value, core):
    return jnp.where(core == 0, value[:, :CH], value[:, CH:])


def pack_body(query, forget, value, left, gate, outgate, conv_out, rec_out, jump, out):
    whole = (query, value, left, outgate)
    split = (forget, forget, gate, gate)
    lane = lax.broadcasted_iota(jnp.int32, (8, CH), 1)
    for c in range(NC):
        half = slice(c * CH, (c + 1) * CH)
        row = jnp.broadcast_to(jump[c : c + 1], (8, CH))
        high = row.astype(bf16).astype(f32)
        first = lax.broadcasted_iota(jnp.int32, (8, CH), 0)
        jumps = jnp.where(first == 0, high, row - high).astype(bf16)
        for x in range(NX):
            to = NC * x + c
            out[to, :CHUNK] = whole[x][:, half]
            rows = split[x][:, half].astype(f32)
            turned = pltpu.roll(rows[8:], CH // 2, 1)
            keep = lane < CH // 2 if x % 2 == 0 else lane >= CH // 2
            out[to, CHUNK:COLUMN_ROWS] = jnp.where(keep, rows[:8], turned).astype(bf16)
            out[to, COLUMN_ROWS : COLUMN_ROWS + CHUNK] = conv_out[:, half]
            out[to, COLUMN_ROWS + CHUNK : COLUMN_ROWS + OUT_ROWS] = rec_out[:, half]
            out[to, COLUMN_ROWS + OUT_ROWS :] = jumps


def norm_body(tokens, gain, out):
    features = tokens[...].astype(f32)
    normed = (
        features
        * lax.rsqrt(jnp.mean(features * features, axis=1, keepdims=True) + norm_eps)
        * gain[...]
    ).astype(bf16)
    for k in range(NX * NY):
        out[k] = normed


def weight_body(own, columns, half, weight):
    blocks = NX * NC
    step = blocks * CHUNK
    for z in range(NZ):
        at = z * step
        piece = columns[z * blocks : (z + 1) * blocks]
        weight[at : at + step, :CH] = piece[:, :CHUNK].reshape(step, CH)
        packed = piece[:, CHUNK:].reshape(blocks * 8, CH).astype(f32)
        turned = pltpu.roll(packed, CH // 2, 1).reshape(blocks, 8, CH)
        both = jnp.concatenate([packed.reshape(blocks, 8, CH), turned], axis=1)
        weight[at : at + step, CH:] = both.reshape(step, CH).astype(bf16)
    half[...] = matmul(own[...], weight[...], ((1,), (0,))).astype(bf16)


def project_body(place, other, half, weight, out):
    c = place[3]
    even = lax.rem(place[2], 2) == 0
    result = matmul(other[...], weight[...], ((1,), (0,))).astype(bf16)
    lane = lax.broadcasted_iota(jnp.int32, (HALF, CH), 1)
    keep = (lane < CH // 2) == even
    for x in range(NX):
        rows = slice(x * HALF, (x + 1) * HALF)
        mine, theirs = half[rows], result[rows]
        out[x, pl.ds(pl.multiple_of(c * HALF, HALF), HALF)] = mine[:, :CH]
        out[x, pl.ds(pl.multiple_of((1 - c) * HALF, HALF), HALF)] = theirs[:, :CH]
        mine, theirs = mine[:, CH:].astype(f32), theirs[:, CH:].astype(f32)
        early = jnp.where(c == 0, mine, theirs)
        late = jnp.where(c == 0, theirs, mine)
        out[x, ROWS:] = jnp.where(keep, early, pltpu.roll(late, CH // 2, 1)).astype(bf16)


def joined(pieces, x):
    lane = lax.broadcasted_iota(jnp.int32, (HALF, CH), 1)
    first, second = (pieces[k, ROWS:].astype(f32) for k in (x, x + 1))
    early = jnp.where(lane < CH // 2, first, second)
    late = pltpu.roll(jnp.where(lane < CH // 2, second, first), CH // 2, 1)
    return jnp.concatenate([early, late], axis=0)


def gates_of(pieces, margin, arrived, place):
    at = COLUMN_ROWS + OUT_ROWS
    rows = [arrived[NC * place[2] + k, at : at + 8].astype(f32) for k in range(NC)]
    jump = jnp.concatenate([r[:1] + r[1:2] for r in rows], axis=1)
    keys = own_half(margin[...], place[3]) * sigmoid(-joined(pieces, 0))
    log_forget = jnp.log1p(-keys)
    row = lax.broadcasted_iota(jnp.int32, (BLOCK, BLOCK), 0)
    col = lax.broadcasted_iota(jnp.int32, (BLOCK, BLOCK), 1)
    causal = row >= col
    lower = jnp.where(causal, 1.0, 0.0)
    running = []
    for n in range(ROWS // BLOCK):
        jumps = jump[:, n * BLOCK : (n + 1) * BLOCK]
        jumped = jnp.sum(jnp.where(causal, jumps, 0.0), axis=1, keepdims=True)
        part = log_forget[n * BLOCK : (n + 1) * BLOCK]
        running.append(matmul(lower, part, ((1,), (0,)), HIGH) + jumped)
    return keys, running, causal


def state_body(place, pieces, margin, arrived, packed, tail):
    keys, running, _ = gates_of(pieces, margin, arrived, place)
    inputs = pieces[1, :ROWS]
    state = jnp.zeros((CH, CH), f32)
    decay = jnp.zeros((1, CH), f32)
    for n in range(ROWS // BLOCK):
        at = slice(n * BLOCK, (n + 1) * BLOCK)
        final = running[n][BLOCK - 1 : BLOCK]
        final_keys = (keys[at] * jnp.exp(final - running[n])).astype(bf16)
        state = state * jnp.exp(final) + matmul(inputs[at], final_keys, ((0,), (0,)))
        decay = decay + final
    high = decay.astype(bf16).astype(f32)
    low = decay - high
    first = lax.broadcasted_iota(jnp.int32, (8, CH), 0)
    sent = jnp.where(first == 0, high, jnp.where(first == 1, low, 0.0)).astype(bf16)
    for x in range(NX):
        packed[x, :OWN] = state[x * OWN : (x + 1) * OWN].astype(bf16)
        packed[x, OWN:] = sent
    tail[:, :CH] = pieces[2, ROWS - HALO : ROWS]
    tail[:, CH:] = joined(pieces, 2)[ROWS - HALO :].astype(bf16)


def local_body(place, pieces, margin, arrived, inner, decayed):
    keys, running, causal = gates_of(pieces, margin, arrived, place)
    queries = silu(pieces[0, :ROWS].astype(f32))
    inputs = pieces[1, :ROWS]
    state = jnp.zeros((CH, CH), f32)
    before = jnp.zeros((1, CH), f32)
    for n in range(ROWS // BLOCK):
        at = slice(n * BLOCK, (n + 1) * BLOCK)
        final = running[n][BLOCK - 1 : BLOCK]
        scaled = queries[at] * jnp.exp(running[n])
        scaled_keys = (keys[at] * jnp.exp(-running[n])).astype(bf16)
        final_keys = (keys[at] * jnp.exp(final - running[n])).astype(bf16)
        scores = matmul(scaled.astype(bf16), scaled_keys, ((1,), (1,)))
        scores = jnp.where(causal, scores, 0.0).astype(bf16)
        inner[at] = matmul(scores, inputs[at], ((1,), (0,))) + matmul(
            scaled.astype(bf16), state.astype(bf16), ((1,), (1,))
        )
        decayed[at] = (scaled * jnp.exp(before)).astype(bf16)
        state = state * jnp.exp(final) + matmul(inputs[at], final_keys, ((0,), (0,)))
        before = before + final


def unpacked(block):
    wide = block.astype(f32)
    return wide[OWN : OWN + 1] + wide[OWN + 1 : OWN + 2], wide[:OWN]


def slab_body(parts, total):
    state = jnp.zeros((OWN, CH), f32)
    decay = jnp.zeros((1, CH), f32)
    for x in range(NX):
        step, add = unpacked(parts[x])
        state = state * jnp.exp(step) + add
        decay = decay + step
    high = decay.astype(bf16).astype(f32)
    low = decay - high
    first = lax.broadcasted_iota(jnp.int32, (8, CH), 0)
    tail = jnp.where(first == 0, high, jnp.where(first == 1, low, 0.0)).astype(bf16)
    for z in range(NZ):
        total[z, :OWN] = state.astype(bf16)
        total[z, OWN:] = tail


def bridge_body(place, slabs, parts, sums, out):
    mine = NQ * place[0] + place[1]
    own = NY * place[3] + place[4]
    state = jnp.zeros((OWN, CH), f32)
    for z in range(NZ):
        step, add = unpacked(slabs[z])
        state = jnp.where(z < mine, state * jnp.exp(step) + add, state)
    row = lax.broadcasted_iota(jnp.int32, (8, CH), 0)
    packed = []
    for k in range(2):
        value = sums[:, k * CH : (k + 1) * CH]
        high = value.astype(bf16).astype(f32)
        middle = (value - high).astype(bf16).astype(f32)
        low = value - high - middle
        packed.append(jnp.where(row < 2, high, jnp.where(row < 4, middle, low)))
    packed = jnp.concatenate([*packed, jnp.zeros((16, CH), f32)], axis=0)
    for x in range(NX):
        for k in range(NC * NY):
            out[x * NC * NY + k] = jnp.where(k == own, state, packed).astype(bf16)
        step, add = unpacked(parts[x])
        state = state * jnp.exp(step) + add


def conv_body(place, pieces, halo, taps, out, sums, gated):
    rim = halo[...].astype(f32)
    gated[:HALO] = rim[:, :CH] * sigmoid(rim[:, CH:])
    gated[HALO:] = pieces[2, :ROWS].astype(f32) * sigmoid(joined(pieces, 2))
    own_taps = own_half(taps[...], place[3])
    for n in range(ROWS // BLOCK):
        total = jnp.zeros((BLOCK, CH), f32)
        for j in range(TAPS):
            at = n * BLOCK + HALO - TAPS + 1 + j
            total = total + gated[at : at + BLOCK] * own_taps[j : j + 1]
        out[n * BLOCK : (n + 1) * BLOCK] = total.astype(bf16)
    values = out[...].astype(f32)
    ones = jnp.ones((8, CH), f32)
    first_sum = matmul(ones, values, ((1,), (1,)), HIGH)
    second_sum = matmul(ones, values * values, ((1,), (1,)), HIGH)
    row = lax.broadcasted_iota(jnp.int32, (8, ROWS), 0)
    sums[...] = jnp.where(row % 2 == 0, first_sum, second_sum)


def order_body(pieces, weight):
    blocks = NX * NC
    step = blocks * CHUNK
    for z in range(NZ):
        at = z * step
        piece = pieces[z]
        weight[at : at + step, :CH] = piece[:, :CHUNK].reshape(step, CH)
        weight[at : at + step, CH:] = piece[:, CHUNK:].reshape(step, CH)


def tail_body(
    place, joint, sums, values, gain, bias, inner, decayed, head_gain, pieces, weight, mine, theirs, both
):
    c = place[3]
    group = NC * NY
    own = NY * c + place[4]
    total = jnp.zeros((8, ROWS), f32)
    for k in range(group):
        piece = joint[group * place[2] + k].astype(f32)
        part = jnp.concatenate([piece[:8], piece[8:16]], axis=1)
        total = total + jnp.where(k == own, 0.0, part)
    row = lax.broadcasted_iota(jnp.int32, (8, ROWS), 0)
    total = total + jnp.where(row < 2, sums[...], 0.0)
    row = lax.broadcasted_iota(jnp.int32, (8, CH), 0)
    pick_first = jnp.where((row < 6) & (row % 2 == 0), 1.0 / CONV_CH, 0.0)
    pick_second = jnp.where((row < 6) & (row % 2 == 1), 1.0 / CONV_CH, 0.0)
    mean = matmul(total, pick_first, ((0,), (0,)), HIGH)
    variance = matmul(total, pick_second, ((0,), (0,)), HIGH) - mean * mean
    shifted = (values[...].astype(f32) - mean) * lax.rsqrt(variance + layer_eps)
    both[:, :CH] = silu(shifted * own_half(gain[...], c) + own_half(bias[...], c)).astype(bf16)
    start = jnp.concatenate([joint[group * x + own] for x in range(NX)], axis=0)
    recurrent = inner[...] + matmul(decayed[...], start, ((1,), (1,)))
    scale = lax.rsqrt(jnp.mean(recurrent * recurrent, axis=1, keepdims=True) + norm_eps)
    gate = silu(pieces[3, :ROWS].astype(f32))
    both[:, CH:] = (recurrent * scale * own_half(head_gain[...], c) * gate).astype(bf16)
    for core, out in ((c, mine), (1 - c, theirs)):
        rows = pl.ds(pl.multiple_of(core * HALF, HALF), HALF)
        out[...] = matmul(both[rows], weight[...], ((1,), (1,))).astype(bf16)


def exchanged(x, axes):
    return lax.all_to_all(x, axes, split_axis=0, concat_axis=0, tiled=True)


def per_device(
    tokens,
    input_norm_gain,
    convolution_value_weight,
    convolution_gate_weight,
    depthwise_filter_taps,
    channel_norm_gain,
    channel_norm_bias,
    query_projection_weight,
    forget_gate_weight,
    recurrence_value_weight,
    output_gate_weight,
    forget_floor_margin,
    decay_jump_terms,
    head_norm_gain,
    convolution_output_weight,
    recurrence_output_weight,
):
    place = jnp.stack([lax.axis_index(a) for a in SP_TP]).astype(jnp.int32)
    width = tokens.shape[1]

    payload = kernel_call(
        pack_body, shape((NX * NC, SENT_ROWS, CH), bf16), [VMEM] * 9, near=False
    )(
        query_projection_weight,
        forget_gate_weight,
        recurrence_value_weight,
        convolution_value_weight,
        convolution_gate_weight,
        output_gate_weight,
        convolution_output_weight.T,
        recurrence_output_weight.T,
        decay_jump_terms,
    )
    arrived = exchanged(payload, (X, C))
    copies = kernel_call(
        norm_body, shape((NX * NY, OWN, width), bf16), [VMEM, VMEM], near=False
    )(tokens, input_norm_gain.reshape(1, width))
    own = exchanged(copies, (X, Y)).reshape(NX * HALF, width)
    other = lax.ppermute(own, C, [(0, 1), (1, 0)])
    columns = lax.all_gather(arrived[:, :COLUMN_ROWS], (ZH, ZL), axis=0, tiled=True)
    out_pieces = lax.all_gather(
        arrived[:, COLUMN_ROWS : COLUMN_ROWS + OUT_ROWS], (ZH, ZL), axis=0
    )
    half, weight = kernel_call(
        weight_body,
        (shape((NX * HALF, 2 * CH), bf16), shape((width, 2 * CH), bf16)),
        [VMEM] * 2,
    )(own, columns)
    projected = kernel_call(
        project_body, shape((NX, ROWS + HALF, CH), bf16), [SMEM] + [VMEM] * 3
    )(place, other, half, weight)
    pieces = exchanged(projected, X)

    margin = forget_floor_margin.reshape(1, 2 * CH)
    packed, tail = kernel_call(
        state_body,
        (shape((NX, STATE_ROWS, CH), bf16), shape((HALO, 2 * CH), bf16)),
        [SMEM] + [VMEM] * 3,
    )(place, pieces, margin, arrived)
    inner, decayed = kernel_call(
        local_body,
        (shape((ROWS, CH), f32), shape((ROWS, CH), bf16)),
        [SMEM] + [VMEM] * 3,
    )(place, pieces, margin, arrived)
    parts = exchanged(packed, X)
    slab_copies = kernel_call(
        slab_body, shape((NZ, STATE_ROWS, CH), bf16), [VMEM]
    )(parts)
    slabs = exchanged(slab_copies, (ZH, ZL))
    blocks = NZ * NX
    halo = lax.ppermute(tail, (ZH, ZL, X), [(k, k + 1) for k in range(blocks - 1)])
    convolved, sums = kernel_call(
        conv_body,
        (shape((ROWS, CH), bf16), shape((8, ROWS), f32)),
        [SMEM, VMEM, VMEM, VMEM],
        [pltpu.VMEM((HALO + ROWS, CH), f32)],
    )(place, pieces, halo, depthwise_filter_taps)
    bridge = kernel_call(
        bridge_body, shape((NX * NC * NY, OWN, CH), bf16), [SMEM] + [VMEM] * 3
    )(place, slabs, parts, sums)
    joint = exchanged(bridge, (X, C, Y))
    out_weight = kernel_call(order_body, shape((width, 2 * CH), bf16), [VMEM])(
        out_pieces
    )
    mine, theirs = kernel_call(
        tail_body,
        (shape((HALF, width), bf16), shape((HALF, width), bf16)),
        [SMEM] + [VMEM] * 10,
        [pltpu.VMEM((ROWS, 2 * CH), bf16)],
    )(
        place,
        joint,
        sums,
        convolved,
        channel_norm_gain.reshape(1, 2 * CH),
        channel_norm_bias.reshape(1, 2 * CH),
        inner,
        decayed,
        head_norm_gain.reshape(1, 2 * CH),
        pieces,
        out_weight,
    )
    given = lax.ppermute(theirs, C, [(0, 1), (1, 0)])
    pair_sum = (mine.astype(f32) + given.astype(f32)).astype(bf16)
    pieces = exchanged(pair_sum.reshape(NY, OWN, width), Y)
    return pieces.astype(f32).sum(axis=0).astype(bf16)


def solution(mesh):
    split = Mesh(mesh.devices.reshape(NQ, NZ // NQ, NX, NC, mesh.shape["tp"]), SP_TP)
    return jax.shard_map(
        per_device,
        mesh=split,
        in_specs=(
            P(SP_TP, None),
            P(),
            P(SP, "tp"),
            P(SP, "tp"),
            P(None, "tp"),
            P("tp"),
            P("tp"),
            P(SP, "tp"),
            P(SP, "tp"),
            P(SP, "tp"),
            P(SP, "tp"),
            P("tp"),
            P("tp", SP),
            P("tp"),
            P("tp", SP),
            P("tp", SP),
        ),
        out_specs=P(SP_TP, None),
        check_vma=False,
    )
```

```python
import jax
import jax.numpy as jnp
from jax import lax
from jax.experimental import pallas as pl
from jax.experimental.pallas import tpu as pltpu
from jax.sharding import Mesh
from jax.sharding import PartitionSpec as P


ZH, ZL, X, C, Y = "sp_0", "sp_1", "sp_2", "sp_3", "tp"
SP = (ZH, ZL, X, C)
SP_TP = (ZH, ZL, X, C, Y)
NZ, NQ, NX, NC, NY = 16, 4, 4, 2, 4
CONV_CH = 1024
CH = 128
ROWS = 256
OWN = 32
BLOCK = 64
TAPS = 31
HALO = 32
STATE_ROWS = 40
LIMIT = 16 * 2**20
HALF = 128
CHUNK = 16
COLUMN_ROWS = 24
OUT_ROWS = 32
SENT_ROWS = 64
norm_eps = 1e-06
layer_eps = 1e-05
HIGH = lax.Precision.HIGHEST
bf16 = jnp.bfloat16
f32 = jnp.float32

VMEM = pl.BlockSpec(memory_space=pltpu.VMEM)
SMEM = pl.BlockSpec(memory_space=pltpu.SMEM)


def in_vmem(value, spec):
    if spec is SMEM or not isinstance(value, jax.Array):
        return value
    return pltpu.with_memory_space_constraint(value, pltpu.VMEM)


def kernel_call(body, out, specs, scratch=(), name=None, near=True):
    call = pl.pallas_call(
        body,
        out_shape=jax.tree.map(lambda o: pltpu.VMEM(o.shape, o.dtype), out)
        if near or name == "pack"
        else out,
        in_specs=specs,
        out_specs=jax.tree.map(lambda _: VMEM, out),
        scratch_shapes=scratch,
        compiler_params=pltpu.CompilerParams(vmem_limit_bytes=LIMIT if near else None),
    )
    if not near:
        return call
    return lambda *args: call(*[in_vmem(a, s) for a, s in zip(args, specs)])


def shape(dims, dtype):
    return jax.ShapeDtypeStruct(dims, dtype)


def matmul(a, b, dims, precision=None):
    return lax.dot_general(
        a, b, (dims, ((), ())), precision=precision, preferred_element_type=f32
    )


def sigmoid(v):
    return 1.0 / (1.0 + jnp.exp(-v))


def silu(v):
    return v * sigmoid(v)


def own_half(value, core):
    return jnp.where(core == 0, value[:, :CH], value[:, CH:])


def pack_body(query, forget, value, left, gate, outgate, conv_out, rec_out, jump, out):
    whole = (query, value, left, outgate)
    split = (forget, forget, gate, gate)
    lane = lax.broadcasted_iota(jnp.int32, (8, CH), 1)
    for c in range(NC):
        half = slice(c * CH, (c + 1) * CH)
        row = jnp.broadcast_to(jump[c : c + 1], (8, CH))
        high = row.astype(bf16).astype(f32)
        first = lax.broadcasted_iota(jnp.int32, (8, CH), 0)
        jumps = jnp.where(first == 0, high, row - high).astype(bf16)
        for x in range(NX):
            to = NC * x + c
            out[to, :CHUNK] = whole[x][:, half]
            rows = split[x][:, half].astype(f32)
            turned = pltpu.roll(rows[8:], CH // 2, 1)
            keep = lane < CH // 2 if x % 2 == 0 else lane >= CH // 2
            out[to, CHUNK:COLUMN_ROWS] = jnp.where(keep, rows[:8], turned).astype(bf16)
            out[to, COLUMN_ROWS : COLUMN_ROWS + CHUNK] = conv_out[:, half]
            out[to, COLUMN_ROWS + CHUNK : COLUMN_ROWS + OUT_ROWS] = rec_out[:, half]
            out[to, COLUMN_ROWS + OUT_ROWS :] = jumps


def norm_body(tokens, gain, out):
    features = tokens[...].astype(f32)
    normed = (
        features
        * lax.rsqrt(jnp.mean(features * features, axis=1, keepdims=True) + norm_eps)
        * gain[...]
    ).astype(bf16)
    for k in range(NX * NY):
        out[k] = normed


def weight_body(own, columns, half, weight):
    blocks = NX * NC
    step = blocks * CHUNK
    for z in range(NZ):
        at = z * step
        piece = columns[z * blocks : (z + 1) * blocks]
        weight[at : at + step, :CH] = piece[:, :CHUNK].reshape(step, CH)
        packed = piece[:, CHUNK:].reshape(blocks * 8, CH).astype(f32)
        turned = pltpu.roll(packed, CH // 2, 1).reshape(blocks, 8, CH)
        both = jnp.concatenate([packed.reshape(blocks, 8, CH), turned], axis=1)
        weight[at : at + step, CH:] = both.reshape(step, CH).astype(bf16)
    half[...] = matmul(own[...], weight[...], ((1,), (0,))).astype(bf16)


def project_body(place, other, half, weight, out):
    c = place[3]
    even = lax.rem(place[2], 2) == 0
    result = matmul(other[...], weight[...], ((1,), (0,))).astype(bf16)
    lane = lax.broadcasted_iota(jnp.int32, (HALF, CH), 1)
    keep = (lane < CH // 2) == even
    for x in range(NX):
        rows = slice(x * HALF, (x + 1) * HALF)
        mine, theirs = half[rows], result[rows]
        out[x, pl.ds(pl.multiple_of(c * HALF, HALF), HALF)] = mine[:, :CH]
        out[x, pl.ds(pl.multiple_of((1 - c) * HALF, HALF), HALF)] = theirs[:, :CH]
        mine, theirs = mine[:, CH:].astype(f32), theirs[:, CH:].astype(f32)
        early = jnp.where(c == 0, mine, theirs)
        late = jnp.where(c == 0, theirs, mine)
        out[x, ROWS:] = jnp.where(keep, early, pltpu.roll(late, CH // 2, 1)).astype(bf16)


def joined(pieces, x):
    lane = lax.broadcasted_iota(jnp.int32, (HALF, CH), 1)
    first, second = (pieces[k, ROWS:].astype(f32) for k in (x, x + 1))
    early = jnp.where(lane < CH // 2, first, second)
    late = pltpu.roll(jnp.where(lane < CH // 2, second, first), CH // 2, 1)
    return jnp.concatenate([early, late], axis=0)


def gates_of(pieces, margin, arrived, place):
    at = COLUMN_ROWS + OUT_ROWS
    rows = [arrived[NC * place[2] + k, at : at + 8].astype(f32) for k in range(NC)]
    jump = jnp.concatenate([r[:1] + r[1:2] for r in rows], axis=1)
    keys = own_half(margin[...], place[3]) * sigmoid(-joined(pieces, 0))
    log_forget = jnp.log1p(-keys)
    row = lax.broadcasted_iota(jnp.int32, (BLOCK, BLOCK), 0)
    col = lax.broadcasted_iota(jnp.int32, (BLOCK, BLOCK), 1)
    causal = row >= col
    lower = jnp.where(causal, 1.0, 0.0)
    running = []
    for n in range(ROWS // BLOCK):
        jumps = jump[:, n * BLOCK : (n + 1) * BLOCK]
        jumped = jnp.sum(jnp.where(causal, jumps, 0.0), axis=1, keepdims=True)
        part = log_forget[n * BLOCK : (n + 1) * BLOCK]
        running.append(matmul(lower, part, ((1,), (0,)), HIGH) + jumped)
    return keys, running, causal


def state_body(place, pieces, margin, arrived, packed, tail):
    keys, running, _ = gates_of(pieces, margin, arrived, place)
    inputs = pieces[1, :ROWS]
    state = jnp.zeros((CH, CH), f32)
    decay = jnp.zeros((1, CH), f32)
    for n in range(ROWS // BLOCK):
        at = slice(n * BLOCK, (n + 1) * BLOCK)
        final = running[n][BLOCK - 1 : BLOCK]
        final_keys = (keys[at] * jnp.exp(final - running[n])).astype(bf16)
        state = state * jnp.exp(final) + matmul(inputs[at], final_keys, ((0,), (0,)))
        decay = decay + final
    high = decay.astype(bf16).astype(f32)
    low = decay - high
    first = lax.broadcasted_iota(jnp.int32, (8, CH), 0)
    sent = jnp.where(first == 0, high, jnp.where(first == 1, low, 0.0)).astype(bf16)
    for x in range(NX):
        packed[x, :OWN] = state[x * OWN : (x + 1) * OWN].astype(bf16)
        packed[x, OWN:] = sent
    tail[:, :CH] = pieces[2, ROWS - HALO : ROWS]
    tail[:, CH:] = joined(pieces, 2)[ROWS - HALO :].astype(bf16)


def local_body(place, pieces, margin, arrived, inner, decayed):
    keys, running, causal = gates_of(pieces, margin, arrived, place)
    queries = silu(pieces[0, :ROWS].astype(f32))
    inputs = pieces[1, :ROWS]
    state = jnp.zeros((CH, CH), f32)
    before = jnp.zeros((1, CH), f32)
    for n in range(ROWS // BLOCK):
        at = slice(n * BLOCK, (n + 1) * BLOCK)
        final = running[n][BLOCK - 1 : BLOCK]
        scaled = queries[at] * jnp.exp(running[n])
        scaled_keys = (keys[at] * jnp.exp(-running[n])).astype(bf16)
        final_keys = (keys[at] * jnp.exp(final - running[n])).astype(bf16)
        scores = matmul(scaled.astype(bf16), scaled_keys, ((1,), (1,)))
        scores = jnp.where(causal, scores, 0.0).astype(bf16)
        inner[at] = matmul(scores, inputs[at], ((1,), (0,))) + matmul(
            scaled.astype(bf16), state.astype(bf16), ((1,), (1,))
        )
        decayed[at] = (scaled * jnp.exp(before)).astype(bf16)
        state = state * jnp.exp(final) + matmul(inputs[at], final_keys, ((0,), (0,)))
        before = before + final


def unpacked(block):
    wide = block.astype(f32)
    return wide[OWN : OWN + 1] + wide[OWN + 1 : OWN + 2], wide[:OWN]


def slab_body(parts, total):
    state = jnp.zeros((OWN, CH), f32)
    decay = jnp.zeros((1, CH), f32)
    for x in range(NX):
        step, add = unpacked(parts[x])
        state = state * jnp.exp(step) + add
        decay = decay + step
    high = decay.astype(bf16).astype(f32)
    low = decay - high
    first = lax.broadcasted_iota(jnp.int32, (8, CH), 0)
    tail = jnp.where(first == 0, high, jnp.where(first == 1, low, 0.0)).astype(bf16)
    for z in range(NZ):
        total[z, :OWN] = state.astype(bf16)
        total[z, OWN:] = tail


def bridge_body(place, slabs, parts, sums, paired, out):
    mine = NQ * place[0] + place[1]
    own = place[4]
    total = sums[...] + paired[...]
    state = jnp.zeros((OWN, CH), f32)
    for z in range(NZ):
        step, add = unpacked(slabs[z])
        state = jnp.where(z < mine, state * jnp.exp(step) + add, state)
    row = lax.broadcasted_iota(jnp.int32, (8, CH), 0)
    packed = []
    for k in range(2):
        value = total[:, k * CH : (k + 1) * CH]
        high = value.astype(bf16).astype(f32)
        middle = (value - high).astype(bf16).astype(f32)
        low = value - high - middle
        packed.append(jnp.where(row < 2, high, jnp.where(row < 4, middle, low)))
    packed = jnp.concatenate([*packed, jnp.zeros((16, CH), f32)], axis=0)
    for x in range(NX):
        for k in range(NY):
            out[x * NY + k] = jnp.where(k == own, state, packed).astype(bf16)
        step, add = unpacked(parts[x])
        state = state * jnp.exp(step) + add


def conv_body(place, pieces, halo, taps, out, sums, gated):
    rim = halo[...].astype(f32)
    gated[:HALO] = rim[:, :CH] * sigmoid(rim[:, CH:])
    gated[HALO:] = pieces[2, :ROWS].astype(f32) * sigmoid(joined(pieces, 2))
    own_taps = own_half(taps[...], place[3])
    for n in range(ROWS // BLOCK):
        total = jnp.zeros((BLOCK, CH), f32)
        for j in range(TAPS):
            at = n * BLOCK + HALO - TAPS + 1 + j
            total = total + gated[at : at + BLOCK] * own_taps[j : j + 1]
        out[n * BLOCK : (n + 1) * BLOCK] = total.astype(bf16)
    values = out[...].astype(f32)
    ones = jnp.ones((8, CH), f32)
    first_sum = matmul(ones, values, ((1,), (1,)), HIGH)
    second_sum = matmul(ones, values * values, ((1,), (1,)), HIGH)
    row = lax.broadcasted_iota(jnp.int32, (8, ROWS), 0)
    sums[...] = jnp.where(row % 2 == 0, first_sum, second_sum)


def order_body(pieces, weight):
    blocks = NX * NC
    step = blocks * CHUNK
    for z in range(NZ):
        at = z * step
        piece = pieces[z]
        weight[at : at + step, :CH] = piece[:, :CHUNK].reshape(step, CH)
        weight[at : at + step, CH:] = piece[:, CHUNK:].reshape(step, CH)


def tail_body(
    place, joint, sums, paired, values, gain, bias, inner, decayed, head_gain, pieces, weight, theirs, both
):
    c = place[3]
    group = NY
    own = place[4]
    total = jnp.zeros((8, ROWS), f32)
    for k in range(group):
        piece = joint[group * place[2] + k].astype(f32)
        part = jnp.concatenate([piece[:8], piece[8:16]], axis=1)
        total = total + jnp.where(k == own, 0.0, part)
    row = lax.broadcasted_iota(jnp.int32, (8, ROWS), 0)
    total = total + jnp.where(row < 2, sums[...] + paired[...], 0.0)
    row = lax.broadcasted_iota(jnp.int32, (8, CH), 0)
    pick_first = jnp.where((row < 6) & (row % 2 == 0), 1.0 / CONV_CH, 0.0)
    pick_second = jnp.where((row < 6) & (row % 2 == 1), 1.0 / CONV_CH, 0.0)
    mean = matmul(total, pick_first, ((0,), (0,)), HIGH)
    variance = matmul(total, pick_second, ((0,), (0,)), HIGH) - mean * mean
    shifted = (values[...].astype(f32) - mean) * lax.rsqrt(variance + layer_eps)
    both[:, :CH] = silu(shifted * own_half(gain[...], c) + own_half(bias[...], c)).astype(bf16)
    start = jnp.concatenate([joint[group * x + own] for x in range(NX)], axis=0)
    recurrent = inner[...] + matmul(decayed[...], start, ((1,), (1,)))
    scale = lax.rsqrt(jnp.mean(recurrent * recurrent, axis=1, keepdims=True) + norm_eps)
    gate = silu(pieces[3, :ROWS].astype(f32))
    both[:, CH:] = (recurrent * scale * own_half(head_gain[...], c) * gate).astype(bf16)
    rows = pl.ds(pl.multiple_of((1 - c) * HALF, HALF), HALF)
    theirs[...] = matmul(both[rows], weight[...], ((1,), (1,))).astype(bf16)


def mine_body(place, both, weight, mine):
    rows = pl.ds(pl.multiple_of(place[3] * HALF, HALF), HALF)
    mine[...] = matmul(both[rows], weight[...], ((1,), (1,)))


def exchanged(x, axes):
    return lax.all_to_all(x, axes, split_axis=0, concat_axis=0, tiled=True)


def per_device(
    tokens,
    input_norm_gain,
    convolution_value_weight,
    convolution_gate_weight,
    depthwise_filter_taps,
    channel_norm_gain,
    channel_norm_bias,
    query_projection_weight,
    forget_gate_weight,
    recurrence_value_weight,
    output_gate_weight,
    forget_floor_margin,
    decay_jump_terms,
    head_norm_gain,
    convolution_output_weight,
    recurrence_output_weight,
):
    place = jnp.stack([lax.axis_index(a) for a in SP_TP]).astype(jnp.int32)
    width = tokens.shape[1]

    payload = kernel_call(
        pack_body, shape((NX * NC, SENT_ROWS, CH), bf16), [VMEM] * 9, name="pack", near=False
    )(
        query_projection_weight,
        forget_gate_weight,
        recurrence_value_weight,
        convolution_value_weight,
        convolution_gate_weight,
        output_gate_weight,
        convolution_output_weight.T,
        recurrence_output_weight.T,
        decay_jump_terms,
    )
    arrived = exchanged(payload, (X, C))
    copies = kernel_call(
        norm_body, shape((NX * NY, OWN, width), bf16), [VMEM, VMEM], name="norm", near=False
    )(tokens, input_norm_gain.reshape(1, width))
    own = exchanged(copies, (X, Y)).reshape(NX * HALF, width)
    other = lax.ppermute(own, C, [(0, 1), (1, 0)])
    columns = lax.all_gather(arrived[:, :COLUMN_ROWS], (ZH, ZL), axis=0, tiled=True)
    out_pieces = lax.all_gather(
        arrived[:, COLUMN_ROWS : COLUMN_ROWS + OUT_ROWS], (ZH, ZL), axis=0
    )
    half, weight = kernel_call(
        weight_body,
        (shape((NX * HALF, 2 * CH), bf16), shape((width, 2 * CH), bf16)),
        [VMEM] * 2,
        name="weight",
    )(own, columns)
    projected = kernel_call(
        project_body,
        shape((NX, ROWS + HALF, CH), bf16),
        [SMEM] + [VMEM] * 3,
        name="project",
    )(place, other, half, weight)
    pieces = exchanged(projected, X)

    margin = forget_floor_margin.reshape(1, 2 * CH)
    packed, tail = kernel_call(
        state_body,
        (shape((NX, STATE_ROWS, CH), bf16), shape((HALO, 2 * CH), bf16)),
        [SMEM] + [VMEM] * 3,
        name="state",
    )(place, pieces, margin, arrived)
    inner, decayed = kernel_call(
        local_body,
        (shape((ROWS, CH), f32), shape((ROWS, CH), bf16)),
        [SMEM] + [VMEM] * 3,
        name="local",
    )(place, pieces, margin, arrived)
    parts = exchanged(packed, X)
    slab_copies = kernel_call(
        slab_body, shape((NZ, STATE_ROWS, CH), bf16), [VMEM], name="slab"
    )(parts)
    slabs = exchanged(slab_copies, (ZH, ZL))
    blocks = NZ * NX
    halo = lax.ppermute(tail, (ZH, ZL, X), [(k, k + 1) for k in range(blocks - 1)])
    convolved, sums = kernel_call(
        conv_body,
        (shape((ROWS, CH), bf16), shape((8, ROWS), f32)),
        [SMEM, VMEM, VMEM, VMEM],
        [pltpu.VMEM((HALO + ROWS, CH), f32)],
        name="conv",
    )(place, pieces, halo, depthwise_filter_taps)
    paired = lax.ppermute(sums, C, [(0, 1), (1, 0)])
    bridge = kernel_call(
        bridge_body, shape((NX * NY, OWN, CH), bf16), [SMEM] + [VMEM] * 4, name="bridge"
    )(place, slabs, parts, sums, paired)
    joint = exchanged(bridge, (X, Y))
    out_weight = kernel_call(order_body, shape((width, 2 * CH), bf16), [VMEM], name="order")(
        out_pieces
    )
    theirs, both = kernel_call(
        tail_body,
        (shape((HALF, width), bf16), shape((ROWS, 2 * CH), bf16)),
        [SMEM] + [VMEM] * 11,
        name="tail",
    )(
        place,
        joint,
        sums,
        paired,
        convolved,
        channel_norm_gain.reshape(1, 2 * CH),
        channel_norm_bias.reshape(1, 2 * CH),
        inner,
        decayed,
        head_norm_gain.reshape(1, 2 * CH),
        pieces,
        out_weight,
    )
    given = lax.ppermute(theirs, C, [(0, 1), (1, 0)])
    mine = kernel_call(mine_body, shape((HALF, width), f32), [SMEM] + [VMEM] * 2, name="mine")(
        place, both, out_weight
    )
    pair_sum = (mine + given.astype(f32)).astype(bf16)
    pieces = exchanged(pair_sum.reshape(NY, OWN, width), Y)
    return pieces.astype(f32).sum(axis=0).astype(bf16)


def solution(mesh):
    split = Mesh(mesh.devices.reshape(NQ, NZ // NQ, NX, NC, mesh.shape["tp"]), SP_TP)
    return jax.shard_map(
        per_device,
        mesh=split,
        in_specs=(
            P(SP_TP, None),
            P(),
            P(SP, "tp"),
            P(SP, "tp"),
            P(None, "tp"),
            P("tp"),
            P("tp"),
            P(SP, "tp"),
            P(SP, "tp"),
            P(SP, "tp"),
            P(SP, "tp"),
            P("tp"),
            P("tp", SP),
            P("tp"),
            P("tp", SP),
            P("tp", SP),
        ),
        out_specs=P(SP_TP, None),
        check_vma=False,
    )
```
